32 devices in a mesh: ep: 4 (over y, x), tp: 8 (over z, core).
Axes of the slice: x: 2, y: 2, z: 4, core: 2. Of those that a mesh axis runs over, the one named last changes fastest.
Arguments:
- tokens: bfloat16 [96, 4096], P('ep'), may hold values from -6 to 6
- norm_gain: float32 [4096], replicated, may hold values from 0.1 to 1.9
- w_query: bfloat16 [4096, 2048], P('ep', 'tp'), may hold values from -0.09375 to 0.09375
- w_forget: bfloat16 [4096, 2048], P('ep', 'tp'), may hold values from -0.09375 to 0.09375
- w_input: bfloat16 [4096, 2048], P('ep', 'tp'), may hold values from -0.09375 to 0.09375
- w_outgate: bfloat16 [4096, 2048], P('ep', 'tp'), may hold values from -0.09375 to 0.09375
- forget_floor: float32 [2048], P('tp'), may hold values from 0.3 to 0.95
- head_gain: float32 [2048], P('tp'), may hold values from 0.1 to 1.9
- recurrent_state: float32 [96, 16, 128, 128], P('ep', 'tp'), may hold values from -2.4 to 2.4
- w_output: bfloat16 [2048, 4096], P('tp', 'ep'), may hold values from -0.125 to 0.125
- ffn_gain: float32 [4096], replicated, may hold values from 0.1 to 1.9
- w_router: bfloat16 [4096, 8], replicated, may hold values from -0.09375 to 0.09375
- routes: int32 [96, 2], P('ep'), may hold values from 0 to 7, all different within a row; in each aligned block of 24 rows (0 to 23, 24 to 47, ...) at most 12 rows name the same one
- expert_gate: bfloat16 [8, 4096, 2816], P('ep', None, 'tp'), may hold values from -0.09375 to 0.09375
- expert_up: bfloat16 [8, 4096, 2816], P('ep', None, 'tp'), may hold values from -0.09375 to 0.09375
- expert_down: bfloat16 [8, 2816, 4096], P('ep', 'tp'), may hold values from -0.109375 to 0.109375
- shared_gate_w: bfloat16 [4096, 2816], P('ep', 'tp'), may hold values from -0.09375 to 0.09375
- shared_up_w: bfloat16 [4096, 2816], P('ep', 'tp'), may hold values from -0.09375 to 0.09375
- shared_down_w: bfloat16 [2816, 4096], P('tp', 'ep'), may hold values from -0.109375 to 0.109375
- branch_gate: bfloat16 [4096], replicated, may hold values from -0.09375 to 0.09375
Outputs:
- layer_out: bfloat16 [96, 4096], P('ep', 'tp')
- new_state: float32 [96, 16, 128, 128], P('ep', 'tp')
The draws below stay inside these ranges and needn't reach their ends.
Inputs may be any that keep to these rules, and one draw needn't show every extreme that they name: `routes`: each row names 2 different experts. Among the rows of one index of ep, no expert is named more than 12 times, a bound that some block reaches.
All inputs are finite; a program needn't handle non-finite values.
Results may differ from the reference program's by a relative error of at most 0.025.
Values may be sent and summed in bfloat16 or wider, within the bound.
No kernel may reach another device: no remote copies, remote signals or barrier semaphores. Data moves between devices by JAX's collectives and lax.ppermute only.
A program may use at most 64 MiB of HBM per device.

```python
import math
import jax
import jax.numpy as jnp
import numpy as np
from jax import lax

D = 4096
HEAD_DIM = 128
HEADS = 16
HGW = 2048
FF = 2816
SFF = 2816
EXPERTS = 8
TOP_K = 2
B_GRP = 24
TOKENS = 96
CAP = 12
N_EP = 4


def shard_levels(stream_key, shape, split, low, largest):
    def one(position, blocks):
        draws = jax.random.uniform(jax.random.fold_in(jax.random.fold_in(stream_key, 6), position), (blocks,), jnp.float32, low / len(split), largest / len(split))
        return jnp.repeat(jnp.exp(draws), shape[position] // blocks).reshape((-1,) + (1,) * (len(shape) - position - 1))

    level = one(*split[0])
    for cut in split[1:]:
        level = level * one(*cut)
    return level


def routed_block(rng, own, number, rows, amount, top, bound, slope):
    ranking = jax.random.permutation(rng, amount)
    crowded, ordinary = load_shares(amount, rows * top, bound, slope, True), load_shares(amount, rows * top, bound, slope, False)
    places = jnp.arange(amount)

    def named(tallies, offset_by):
        used = int((tallies > 0).sum())
        fixed = max(1, used // 4)
        moved = fixed + (places - fixed + offset_by * (used - fixed)) % max(1, amount - fixed)
        return jnp.zeros((amount,), jnp.int32).at[ranking[jnp.where(places < fixed, places, moved)]].set(jnp.asarray(tallies, jnp.int32))

    tallies = jnp.where(number % 4 == 0, named(crowded, number // 4), named(ordinary, number - number // 4 - 1))
    mixed = jax.random.permutation(jax.random.fold_in(own, 3), amount)
    giver, receiver = mixed[0:amount // 2 * 2:2], mixed[1:amount // 2 * 2:2]
    room = jnp.minimum(tallies[giver] - 1, bound - tallies[receiver]) // 2
    room = jnp.where((giver == ranking[0]) | (receiver == ranking[0]) | (tallies[receiver] == 0), 0, jnp.maximum(room, 0))
    moved = jax.random.randint(jax.random.fold_in(own, 4), (amount // 2,), 0, 1 << 20) % (room + 1)
    tallies = tallies.at[giver].add(-moved).at[receiver].add(moved)
    labels = jnp.searchsorted(jnp.cumsum(tallies), jnp.arange(rows * top), side="right").astype(jnp.int32)
    grid = labels.reshape(top, rows).T
    grid = grid[jax.random.permutation(jax.random.fold_in(own, 1), rows)]
    offset_by = jax.random.randint(jax.random.fold_in(own, 2), (rows, 1), 0, top)
    return jnp.take_along_axis(grid, (jnp.arange(top)[None, :] + offset_by) % top, axis=1)


def load_shares(amount, total, limit, slope, full):
    portions = [(1 << 20) // math.isqrt(standing ** slope) + 1 for standing in range(1, amount + 1)]
    largest = limit if full else min(limit, max(-(-total // amount), total * portions[0] // sum(portions)))
    least = 1 if total - largest >= amount - 1 else 0
    counts, spare = [largest] + [least] * (amount - 1), total - largest - least * (amount - 1)
    while spare > 0:
        candidates = [i for i in range(1, amount) if counts[i] < largest] or [i for i in range(1, amount) if counts[i] < limit]
        whole, budget = sum([portions[i] for i in candidates]), spare
        for i in candidates:
            addition = min(limit - counts[i], max(1, budget * portions[i] // whole), spare)
            counts[i] = counts[i] + addition
            spare = spare - addition
    return np.array(counts)


def bell_draw(own_key, shape, scale, most, cuts=(), kind=jnp.bfloat16):
    drawn = scale * jax.random.normal(own_key, shape, jnp.float32)
    if cuts:
        drawn = drawn * shard_levels(own_key, shape, cuts, -0.22, 0.18)
    return jnp.clip(drawn, -most, most).astype(kind)


def setup_inputs(seed: int = 0) -> dict:
    splits = jax.random.split(jax.random.key(seed), 21)
    tokens = bell_draw(splits[0], (TOKENS, D), 1.0, 6.0, ((0, 4),))
    norm_gain = jnp.clip(1.0 + 0.18 * jax.random.normal(splits[1], (D,), jnp.float32), 0.1, 1.9)
    w_query = bell_draw(splits[2], (D, HGW), D ** -0.5, 0.09375, ((0, 4), (1, 8)))
    w_forget = bell_draw(splits[3], (D, HGW), D ** -0.5, 0.09375, ((0, 4), (1, 8)))
    w_input = bell_draw(splits[4], (D, HGW), D ** -0.5, 0.09375, ((0, 4), (1, 8)))
    w_outgate = bell_draw(splits[5], (D, HGW), D ** -0.5, 0.09375, ((0, 4), (1, 8)))
    forget_floor = jnp.clip(0.3 + 0.65 * jax.random.uniform(splits[6], (HGW,), jnp.float32) ** shard_levels(splits[6], (HGW,), ((0, 8),), -0.2, 0.2), 0.3, 0.95)
    head_gain = jnp.clip(1.0 + 0.18 * jax.random.normal(splits[7], (HGW,), jnp.float32), 0.1, 1.9)
    recurrent_state = bell_draw(splits[8], (TOKENS, HEADS, HEAD_DIM, HEAD_DIM), 0.3, 2.4, ((0, 4), (1, 8)), jnp.float32)
    w_output = bell_draw(splits[9], (HGW, D), HGW ** -0.5, 0.125, ((0, 8), (1, 4)))
    ffn_gain = jnp.clip(1.0 + 0.18 * jax.random.normal(splits[10], (D,), jnp.float32), 0.1, 1.9)
    w_router = bell_draw(splits[11], (D, EXPERTS), D ** -0.5, 0.09375)
    routes_keys = jax.random.split(jax.random.fold_in(splits[12], 1), TOKENS // B_GRP)
    routes_turns = jax.random.permutation(jax.random.fold_in(splits[12], 3), TOKENS // B_GRP)
    routes = jax.vmap(lambda own, number: routed_block(jax.random.fold_in(splits[12], 2), own, number, B_GRP, EXPERTS, TOP_K, CAP, 2))(routes_keys, routes_turns).reshape((TOKENS, TOP_K))
    expert_gate = bell_draw(splits[13], (EXPERTS, D, FF), D ** -0.5, 0.09375, ((0, 4), (2, 8)))
    expert_up = bell_draw(splits[14], (EXPERTS, D, FF), D ** -0.5, 0.09375, ((0, 4), (2, 8)))
    expert_down = bell_draw(splits[15], (EXPERTS, FF, D), FF ** -0.5, 0.109375, ((0, 4), (1, 8)))
    shared_gate_w = bell_draw(splits[16], (D, SFF), D ** -0.5, 0.09375, ((0, 4), (1, 8)))
    shared_up_w = bell_draw(splits[17], (D, SFF), D ** -0.5, 0.09375, ((0, 4), (1, 8)))
    shared_down_w = bell_draw(splits[18], (SFF, D), SFF ** -0.5, 0.109375, ((0, 8), (1, 4)))
    branch_gate = bell_draw(splits[19], (D,), D ** -0.5, 0.09375)
    return dict(tokens=tokens, norm_gain=norm_gain, w_query=w_query, w_forget=w_forget, w_input=w_input, w_outgate=w_outgate, forget_floor=forget_floor, head_gain=head_gain, recurrent_state=recurrent_state, w_output=w_output, ffn_gain=ffn_gain, w_router=w_router, routes=routes, expert_gate=expert_gate, expert_up=expert_up, expert_down=expert_down, shared_gate_w=shared_gate_w, shared_up_w=shared_up_w, shared_down_w=shared_down_w, branch_gate=branch_gate)


NORM_EPSILON = 1e-06
ROUTED_SCALE = 2.5

def rms_scale(values, gain):
    floats = values.astype(jnp.float32)
    inverse = lax.rsqrt(lax.optimization_barrier(jnp.mean(floats * floats, axis=-1, keepdims=True)) + NORM_EPSILON)
    return (floats * inverse * gain).astype(jnp.bfloat16)

def run_expert(packed):
    rows_in, gate_w, up_w, down_w = packed
    gate_part = jnp.dot(rows_in, gate_w, preferred_element_type=jnp.float32)
    up_part = jnp.dot(rows_in, up_w, preferred_element_type=jnp.float32)
    inner = (jax.nn.silu(gate_part) * up_part).astype(jnp.bfloat16)
    return jnp.dot(inner, down_w, preferred_element_type=jnp.float32).astype(jnp.bfloat16)

def reference(tokens, norm_gain, w_query, w_forget, w_input, w_outgate, forget_floor, head_gain, recurrent_state, w_output, ffn_gain, w_router, routes, expert_gate, expert_up, expert_down, shared_gate_w, shared_up_w, shared_down_w, branch_gate):
    normed = rms_scale(tokens, norm_gain)
    shape = (TOKENS, HEADS, HEAD_DIM)
    query = jnp.dot(normed, w_query, preferred_element_type=jnp.float32).reshape(shape)
    forget_pre = jnp.dot(normed, w_forget, preferred_element_type=jnp.float32).reshape(shape)
    value_in = jnp.dot(normed, w_input, preferred_element_type=jnp.float32).reshape(shape)
    out_gate = jnp.dot(normed, w_outgate, preferred_element_type=jnp.float32)
    floor = forget_floor.reshape(HEADS, HEAD_DIM)
    forget = floor + (1.0 - floor) * jax.nn.sigmoid(forget_pre)
    key_part = (1.0 - floor) * jax.nn.sigmoid(-forget_pre)
    new_state = forget[..., None] * recurrent_state + key_part[..., None] * value_in[:, :, None, :]
    read = jnp.einsum('bhk,bhkv->bhv', jax.nn.silu(query), new_state, precision=lax.Precision.HIGHEST)
    read = read * lax.rsqrt(lax.optimization_barrier(jnp.mean(read * read, axis=-1, keepdims=True)) + NORM_EPSILON)
    mixed_heads = (read.reshape(TOKENS, HEADS * HEAD_DIM) * head_gain * jax.nn.silu(out_gate)).astype(jnp.bfloat16)
    mixer_out = jnp.dot(mixed_heads, w_output, preferred_element_type=jnp.float32)
    hidden = (tokens.astype(jnp.float32) + mixer_out).astype(jnp.bfloat16)
    normed_two = rms_scale(hidden, ffn_gain)
    affinity = jax.nn.sigmoid(jnp.dot(normed_two, w_router, preferred_element_type=jnp.float32))
    chosen = jnp.take_along_axis(affinity, routes.astype(jnp.int32), axis=1)
    route_weights = chosen / lax.optimization_barrier(jnp.sum(chosen, axis=1, keepdims=True)) * ROUTED_SCALE
    groups = routes.astype(jnp.int32).reshape(N_EP, B_GRP * TOP_K)
    onehot = (groups[:, :, None] == jnp.arange(EXPERTS, dtype=jnp.int32)[None, None, :]).astype(jnp.int32)
    earlier = jnp.cumsum(onehot, axis=1) - onehot
    slot = lax.optimization_barrier(jnp.sum(earlier * onehot, axis=2))
    target = groups * CAP + slot
    placing = (target[:, :, None] == jnp.arange(EXPERTS * CAP, dtype=jnp.int32)[None, None, :]).astype(jnp.float32)
    token_slot = lax.optimization_barrier(jnp.sum(placing.reshape(N_EP, B_GRP, TOP_K, EXPERTS * CAP), axis=2))
    grouped = normed_two.reshape(N_EP, B_GRP, D).astype(jnp.float32)
    buffers = jnp.einsum('gbs,gbd->gsd', token_slot, grouped, precision=lax.Precision.HIGHEST)
    buffers = buffers.reshape(N_EP, EXPERTS, CAP, D).transpose(1, 0, 2, 3).reshape(EXPERTS, N_EP * CAP, D)
    outputs = lax.map(run_expert, (buffers.astype(jnp.bfloat16), expert_gate, expert_up, expert_down))
    back = outputs.reshape(EXPERTS, N_EP, CAP, D).transpose(1, 0, 2, 3).reshape(N_EP, EXPERTS * CAP, D)
    per_route = jnp.einsum('grs,gsd->grd', placing, back.astype(jnp.float32), precision=lax.Precision.HIGHEST)
    routed = lax.optimization_barrier(jnp.sum(per_route.reshape(TOKENS, TOP_K, D) * route_weights[:, :, None], axis=1))
    shared_gate = jnp.dot(normed_two, shared_gate_w, preferred_element_type=jnp.float32)
    shared_up = jnp.dot(normed_two, shared_up_w, preferred_element_type=jnp.float32)
    shared_inner = (jax.nn.silu(shared_gate) * shared_up).astype(jnp.bfloat16)
    shared_out = jnp.dot(shared_inner, shared_down_w, preferred_element_type=jnp.float32)
    branch = jax.nn.sigmoid(jnp.dot(normed_two, branch_gate, preferred_element_type=jnp.float32))
    layer_out = (hidden.astype(jnp.float32) + routed + branch[:, None] * shared_out).astype(jnp.bfloat16)
    return (layer_out, new_state)
```

```python
import jax
import jax.numpy as jnp
from jax import lax
from jax.sharding import PartitionSpec as P

NORM_EPSILON = 1e-06
ROUTED_SCALE = 2.5
LANES = 128
F32 = jnp.float32
BF16 = jnp.bfloat16


def dot(a, b):
    return jnp.dot(a, b, preferred_element_type=F32)


def swap(value, axis, size, step):
    return lax.ppermute(value, axis, [(s, s ^ step) for s in range(size)])


def inverse_rms(floats):
    return lax.rsqrt(jnp.mean(floats * floats, axis=-1, keepdims=True) + NORM_EPSILON)


def make_body(n_ep, n_tp):
    n_z = n_tp // 2

    def ep_swap(value, k):
        return swap(value, "ep", n_ep, k) if k else value

    def z_swap(value, m):
        return swap(value, "tp", n_tp, 2 * m) if m else value

    def core_swap(value):
        return swap(value, "tp", n_tp, 1)

    def body(
        tokens, norm_gain, w_query, w_forget, w_input, w_outgate, forget_floor, head_gain,
        recurrent_state, w_output, ffn_gain, w_router, routes, expert_gate, expert_up,
        expert_down, shared_gate_w, shared_up_w, shared_down_w, branch_gate,
    ):
        e = lax.axis_index("ep")
        t = lax.axis_index("tp")
        c = lax.rem(t, 2)
        z = lax.div(t, 2)
        batch, width = tokens.shape
        rows = n_ep * batch
        block = width // n_ep
        half = block // 2
        heads_here, head_size = recurrent_state.shape[1:3]
        channels = heads_here * head_size

        extra = jnp.pad(routes.astype(BF16), ((0, 0), (0, LANES - routes.shape[1])))
        got = []
        for k in range(n_ep):
            piece = lax.dynamic_slice_in_dim(tokens, (e ^ k) * block, block, 1)
            got.append(ep_swap(jnp.concatenate([piece, extra], axis=1), k))
        got = jnp.concatenate(got, axis=0)
        raw = got[:, :block]
        all_routes = got[:, block : block + routes.shape[1]].astype(jnp.int32)
        gain = lax.dynamic_slice_in_dim(norm_gain, e * block, block, 0)
        scaled = (raw.astype(F32) * gain).astype(BF16)
        inv = inverse_rms(tokens.astype(F32))

        parts = jnp.concatenate(
            [dot(scaled, w) for w in (w_query, w_forget, w_input, w_outgate)], axis=1
        )
        total = parts[:batch]
        sent = parts.astype(BF16)
        for k in range(1, n_ep):
            total = total + ep_swap(sent[k * batch : (k + 1) * batch], k).astype(F32)
        total = total * inv
        query, forget_pre, value_in, out_gate = (
            total[:, i * channels : (i + 1) * channels] for i in range(4)
        )
        shape = (batch, heads_here, head_size)
        floor = forget_floor.reshape(heads_here, head_size)
        forget_pre = forget_pre.reshape(shape)
        value_in = value_in.reshape(shape)
        forget = floor + (1.0 - floor) * jax.nn.sigmoid(forget_pre)
        key_part = (1.0 - floor) * jax.nn.sigmoid(-forget_pre)
        new_state = (
            forget[..., None] * recurrent_state + key_part[..., None] * value_in[:, :, None, :]
        )
        activated = jax.nn.silu(query.reshape(shape))
        read = jnp.sum((activated * forget)[..., None] * recurrent_state, axis=2)
        read = read + jnp.sum(activated * key_part, axis=-1, keepdims=True) * value_in
        read = read * inverse_rms(read)
        mixed = (read.reshape(batch, channels) * head_gain * jax.nn.silu(out_gate)).astype(BF16)

        mixed_all = jnp.concatenate([ep_swap(mixed, k) for k in range(n_ep)], axis=0)
        partial = dot(mixed_all, w_output)
        keep = lax.dynamic_slice_in_dim(partial, c * half, half, 1)
        give = lax.dynamic_slice_in_dim(partial, (1 - c) * half, half, 1).astype(BF16)
        keep = keep + core_swap(give).astype(F32)
        sent = keep.astype(BF16)
        for m in range(1, n_z):
            keep = keep + z_swap(sent, m).astype(F32)
        raw_half = lax.dynamic_slice_in_dim(raw, c * half, half, 1)
        hidden_part = (raw_half.astype(F32) + keep).astype(BF16)

        mine = []
        for k in range(n_ep):
            piece = ep_swap(hidden_part, k).reshape(n_ep, batch, half)
            mine.append(jnp.concatenate([piece[j ^ k] for j in range(n_ep)], axis=0))
        mine = jnp.stack(mine)
        both = jnp.stack([mine, core_swap(mine)])
        hidden = jnp.concatenate(
            [both[h ^ c, j ^ e] for j in range(n_ep) for h in range(2)], axis=1
        )

        floats = hidden.astype(F32)
        normed = (floats * inverse_rms(floats) * ffn_gain).astype(BF16)
        experts = w_router.shape[1]
        local = expert_gate.shape[0]
        inner_width = expert_gate.shape[2]
        affinity = jax.nn.sigmoid(dot(normed, w_router))
        picks = all_routes[:, :, None] == jnp.arange(experts, dtype=jnp.int32)[None, None, :]
        chosen = jnp.sum(jnp.where(picks, affinity[:, None, :], 0.0), axis=2)
        weights = chosen / jnp.sum(chosen, axis=1, keepdims=True) * ROUTED_SCALE
        combine = jnp.sum(jnp.where(picks, weights[:, :, None], 0.0), axis=1)
        combine = lax.dynamic_slice_in_dim(combine, e * local, local, 1)
        branch = jax.nn.sigmoid(dot(normed, branch_gate))[:, None]

        own = lax.dynamic_slice_in_dim(normed, e * block, block, 1)
        shared_sent = jnp.concatenate(
            [dot(own, shared_gate_w), dot(own, shared_up_w)], axis=1
        )
        shared_sum = shared_sent
        shared_sent = shared_sent.astype(BF16)
        for k in range(1, n_ep):
            piece = ep_swap(shared_sent, k).reshape(n_ep, batch, -1)
            piece = jnp.concatenate([piece[j ^ k] for j in range(n_ep)], axis=0)
            shared_sum = shared_sum + piece.astype(F32)
        shared_width = shared_gate_w.shape[1]
        shared_inner = jax.nn.silu(shared_sum[:, :shared_width]) * shared_sum[:, shared_width:]
        shared_inner = (shared_inner * branch).astype(BF16)

        final = jnp.zeros((rows, width), F32)
        for x in range(local):
            inner = jax.nn.silu(dot(normed, expert_gate[x])) * dot(normed, expert_up[x])
            inner = (inner * combine[:, x : x + 1]).astype(BF16)
            final = final + dot(inner, expert_down[x])
        shared_out = dot(shared_inner, shared_down_w)
        old = lax.dynamic_slice_in_dim(final, e * block, block, 1)
        final = lax.dynamic_update_slice_in_dim(final, old + shared_out, e * block, 1)

        slice_width = width // n_tp
        final = final.reshape(rows, n_z, 2, slice_width)
        keep = lax.dynamic_index_in_dim(final, c, 2, keepdims=False)
        give = lax.dynamic_index_in_dim(final, 1 - c, 2, keepdims=False).astype(BF16)
        keep = keep + core_swap(give.reshape(rows, -1)).astype(F32).reshape(keep.shape)
        sent = keep.astype(BF16).reshape(rows, -1)
        total = keep[:batch].reshape(batch, -1)
        for k in range(1, n_ep):
            total = total + ep_swap(sent[k * batch : (k + 1) * batch], k).astype(F32)
        sent = total.astype(BF16)
        result = lax.dynamic_slice_in_dim(total, z * slice_width, slice_width, 1)
        for m in range(1, n_z):
            piece = lax.dynamic_slice_in_dim(sent, (z ^ m) * slice_width, slice_width, 1)
            result = result + z_swap(piece, m).astype(F32)
        own_hidden = lax.dynamic_slice(hidden, (0, t * slice_width), (batch, slice_width))
        layer_out = (own_hidden.astype(F32) + result).astype(BF16)
        return layer_out, new_state

    return body


def solution(mesh):
    return jax.shard_map(
        make_body(mesh.shape["ep"], mesh.shape["tp"]),
        mesh=mesh,
        in_specs=(
            P("ep", None),
            P(),
            P("ep", "tp"),
            P("ep", "tp"),
            P("ep", "tp"),
            P("ep", "tp"),
            P("tp"),
            P("tp"),
            P("ep", "tp", None, None),
            P("tp", "ep"),
            P(),
            P(),
            P("ep", None),
            P("ep", None, "tp"),
            P("ep", None, "tp"),
            P("ep", "tp", None),
            P("ep", "tp"),
            P("ep", "tp"),
            P("tp", "ep"),
            P(),
        ),
        out_specs=(P("ep", "tp"), P("ep", "tp", None, None)),
        check_vma=False,
    )
```

```python
import functools

import jax
import jax.numpy as jnp
from jax import lax
from jax.experimental import pallas as pl
from jax.experimental.pallas import tpu as pltpu
from jax.sharding import PartitionSpec as P

NORM_EPSILON = 1e-06
ROUTED_SCALE = 2.5
LANES = 128
F32 = jnp.float32
BF16 = jnp.bfloat16
VMEM = pl.BlockSpec(memory_space=pltpu.VMEM)
HBM = pl.BlockSpec(memory_space=pltpu.HBM)


def dot(a, b):
    return jnp.dot(a, b, preferred_element_type=F32)


def dot_t(a, b):
    return lax.dot_general(a, b, (((1,), (1,)), ((), ())), preferred_element_type=F32)


def silu(x):
    return x * jax.nn.sigmoid(x)


def swap(value, axis, size, step):
    return lax.ppermute(value, axis, [(s, s ^ step) for s in range(size)])


def inverse_rms(floats):
    return lax.rsqrt(jnp.mean(floats * floats, axis=-1, keepdims=True) + NORM_EPSILON)


def lane_slice(index, size):
    return pl.ds(pl.multiple_of(index * size, LANES), size)


def call(body, outs, ins, args, scratch=(), flops=0, limit=24):
    return pl.pallas_call(
        body,
        out_shape=[jax.ShapeDtypeStruct(s, d) for s, d in outs],
        in_specs=ins,
        out_specs=[VMEM] * len(outs),
        scratch_shapes=list(scratch),
        cost_estimate=pl.CostEstimate(flops=flops, bytes_accessed=0, transcendentals=0),
        compiler_params=pltpu.CompilerParams(vmem_limit_bytes=limit << 20),
    )(*args)


def prepare_kernel(n_ep, tokens, routes_t, *outs):
    e = lax.axis_index("ep")
    batch, width = tokens.shape
    block = width // n_ep
    names = lax.broadcasted_iota(jnp.int32, (LANES, batch), 0)
    hit = names == routes_t[0:1, :]
    for j in range(1, routes_t.shape[0]):
        hit = hit | (names == routes_t[j : j + 1, :])
    eye = lax.broadcasted_iota(jnp.int32, (batch, batch), 0) == lax.broadcasted_iota(
        jnp.int32, (batch, batch), 1
    )
    mask = dot_t(
        jnp.where(eye, 1.0, 0.0).astype(BF16), jnp.where(hit, 1.0, 0.0).astype(BF16)
    ).astype(BF16)
    for k, out in enumerate(outs):
        out[:, :block] = tokens[:, lane_slice(e ^ k, block)]
        out[:, block:] = mask


def fetch_kernel(arrays, *refs):
    sources, copied, token, sems = refs[:arrays], refs[-arrays - 2 : -2], refs[-2], refs[-1]
    copies = []
    for source, target in zip(sources, copied, strict=True):
        parts = 4 if source.shape[0] % 4 == 0 else source.shape[0]
        step = source.shape[0] // parts
        for p in range(parts):
            span = pl.ds(p * step, step)
            copies.append(
                pltpu.make_async_copy(source.at[span], target.at[span], sems.at[len(copies)])
            )
    for copy in copies:
        copy.start()
    for copy in copies:
        copy.wait()
    token[...] = jnp.zeros_like(token)


def fetch(arrays, after):
    arrays = [pltpu.with_memory_space_constraint(a, pltpu.HBM) for a in arrays]
    *copied, token = call(
        functools.partial(fetch_kernel, len(arrays)),
        [(a.shape, a.dtype) for a in arrays] + [((8, LANES), F32)],
        [HBM] * len(arrays) + [VMEM],
        (*arrays, after),
        [pltpu.SemaphoreType.DMA((24 * len(arrays),))],
        flops=1 << 26,
        limit=1,
    )
    return copied, token


def inverse_kernel(tokens, router_t, branch, out, router):
    out[...] = jnp.broadcast_to(inverse_rms(tokens[...].astype(F32)), out.shape)
    extra = jnp.broadcast_to(branch[...].astype(F32), (8, branch.shape[1]))
    router[...] = jnp.concatenate([router_t[...].astype(F32), extra], axis=0).astype(BF16)


def project_kernel(n_ep, *refs):
    payloads, gain, weights = refs[:n_ep], refs[n_ep], refs[n_ep + 1 : n_ep + 5]
    own, sent = refs[n_ep + 6], refs[n_ep + 7 :]
    batch = own.shape[0]
    block, channels = weights[0].shape
    row = gain[:, lane_slice(lax.axis_index("ep"), block)]
    scaled = jnp.concatenate([p[:, :block].astype(F32) for p in payloads], axis=0) * row
    scaled = scaled.astype(BF16)
    for i, weight in enumerate(weights):
        part = dot(scaled, weight[...])
        lanes = slice(i * channels, (i + 1) * channels)
        own[:, lanes] = part[:batch]
        for k in range(1, n_ep):
            sent[k - 1][:, lanes] = part[k * batch : (k + 1) * batch].astype(BF16)


def columns_of(value):
    rows, lanes = value.shape
    return jnp.concatenate([value, jnp.zeros((LANES - rows, lanes), F32)], axis=0).T


def read_kernel(n_ep, *refs):
    own, got = refs[0], refs[1:n_ep]
    inverse, floor, head_gain, state = refs[n_ep : n_ep + 4]
    mixed, gates, scratch = refs[n_ep + 4 :]
    batch, heads, size = state.shape[:3]
    channels = heads * size
    total = own[...]
    for g in got:
        total = total + g[...].astype(F32)
    total = total * inverse[:, 0:1]
    query, forget_pre, value, out_gate = (
        total[:, i * channels : (i + 1) * channels] for i in range(4)
    )
    low = floor[...]
    forget = low + (1.0 - low) * jax.nn.sigmoid(forget_pre)
    key = (1.0 - low) * jax.nn.sigmoid(-forget_pre)
    gates[:, :channels] = forget
    gates[:, channels : 2 * channels] = key
    gates[:, 2 * channels :] = value
    active = silu(query)
    weight = columns_of(active * forget)
    for b in range(batch):
        for h in range(heads):
            column = weight[h * size : (h + 1) * size, b : b + 1]
            scratch[b : b + 1, h * size : (h + 1) * size] = jnp.sum(
                column * state[b, h], axis=0, keepdims=True
            )
    scale = head_gain[...] * silu(out_gate)
    for h in range(heads):
        lanes = slice(h * size, (h + 1) * size)
        read = scratch[:, lanes] + value[:, lanes] * jnp.sum(
            active[:, lanes] * key[:, lanes], axis=-1, keepdims=True
        )
        mixed[:, lanes] = (read * inverse_rms(read) * scale[:, lanes]).astype(BF16)


def update_kernel(gates, state, out, token):
    group, heads, size = state.shape[:3]
    channels = heads * size
    forget = columns_of(gates[:, :channels])
    key = columns_of(gates[:, channels : 2 * channels])
    for b in range(group):
        for h in range(heads):
            rows = slice(h * size, (h + 1) * size)
            value = gates[b : b + 1, 2 * channels + h * size : 2 * channels + (h + 1) * size]
            out[b, h] = forget[rows, b : b + 1] * state[b, h] + key[rows, b : b + 1] * value
    token[...] = jnp.zeros_like(token)


def output_kernel(n_ep, *refs):
    mixed, weight, give, keep = refs[:n_ep], refs[n_ep], refs[-2], refs[-1]
    c = lax.rem(lax.axis_index("tp"), 2)
    half = keep.shape[1]
    rows = jnp.concatenate([m[...].astype(F32) for m in mixed], axis=0).astype(BF16)
    give[...] = dot(rows, weight[:, lane_slice(1 - c, half)]).astype(BF16)
    keep[...] = dot(rows, weight[:, lane_slice(c, half)])


def add_kernel(keep, got, out):
    out[...] = (keep[...] + got[...].astype(F32)).astype(BF16)


def hidden_kernel(n_ep, n_z, *refs):
    payloads, keep, core, others = refs[:n_ep], refs[n_ep], refs[n_ep + 1], refs[n_ep + 2 : -2]
    out = refs[-1]
    c = lax.rem(lax.axis_index("tp"), 2)
    half = keep.shape[1]
    total = jnp.concatenate([p[:, lane_slice(c, half)].astype(F32) for p in payloads], axis=0)
    mixed = keep[...] + core[...].astype(F32)
    for other in others:
        mixed = mixed + other[...].astype(F32)
    out[...] = (total + mixed).astype(BF16)


def shared_kernel(mine, other, gain, gate_t, up_t, own, sent):
    c = lax.rem(lax.axis_index("tp"), 2)
    e = lax.axis_index("ep")
    half = mine.shape[1]
    inner, padded = gate_t.shape[0], own.shape[1] // 2
    own[...] = jnp.zeros_like(own)
    total = [None, None]
    for piece, h in ((mine, c), (other, 1 - c)):
        row = gain[:, lane_slice(2 * e + h, half)]
        scaled = (piece[...].astype(F32) * row).astype(BF16)
        for i, weight in enumerate((gate_t, up_t)):
            part = dot_t(scaled, weight[:, lane_slice(h, half)])
            total[i] = part if total[i] is None else total[i] + part
    for i in range(2):
        own[:, i * padded : i * padded + inner] = total[i]
    sent[...] = own[...].astype(BF16)


def expert_kernel(n_ep, *refs):
    pieces, others, payloads = refs[:n_ep], refs[n_ep : 2 * n_ep], refs[2 * n_ep : 3 * n_ep]
    gain, router, gate_buf, up_buf = refs[3 * n_ep : 3 * n_ep + 4]
    inner, scales, own_hidden, x_ref, n_ref = refs[3 * n_ep + 4 :]
    local = gate_buf.shape[0]
    e = lax.axis_index("ep")
    t = lax.axis_index("tp")
    c = lax.rem(t, 2)
    rows, half = pieces[0].shape
    batch = rows // n_ep
    squares = jnp.zeros((rows, half), F32)
    for k in range(n_ep):
        for source, h in ((pieces[k], c), (others[k], 1 - c)):
            floats = source[...].astype(F32)
            floats = jnp.concatenate(
                [floats[(j ^ k) * batch : ((j ^ k) + 1) * batch] for j in range(n_ep)], axis=0
            )
            squares = squares + floats * floats
            x_ref[:, lane_slice(2 * (e ^ k) + h, half)] = floats
    width = x_ref.shape[1]
    inv = lax.rsqrt(jnp.sum(squares, axis=-1, keepdims=True) / width + NORM_EPSILON)
    own_hidden[...] = x_ref[:batch, lane_slice(t, own_hidden.shape[1])]
    n_ref[...] = (x_ref[...] * inv * gain[...]).astype(BF16)
    scores = jax.nn.sigmoid(dot_t(n_ref[...], router[...]))
    experts = router.shape[0] - 8
    lane = lax.broadcasted_iota(jnp.int32, scores.shape, 1)
    block = payloads[0].shape[1] - LANES
    mask = jnp.concatenate([p[:, block:].astype(F32) for p in payloads], axis=0)
    chosen = jnp.where(mask[:, : router.shape[0]] > 0.5, scores, 0.0)
    weights = chosen / jnp.sum(chosen, axis=1, keepdims=True) * ROUTED_SCALE
    branch = jnp.sum(jnp.where(lane == experts, scores, 0.0), axis=1, keepdims=True)
    spread = lax.broadcasted_iota(jnp.int32, scales.shape, 1)
    scales[...] = jnp.where(spread == 0, inv, branch)
    for i in range(local):
        combine = jnp.sum(jnp.where(lane == e * local + i, weights, 0.0), axis=1, keepdims=True)
        gate = dot_t(n_ref[...], gate_buf[i])
        up = dot_t(n_ref[...], up_buf[i])
        inner[i] = (silu(gate) * up * combine).astype(BF16)


def down_kernel(n_ep, n_z, mine, inner, *refs):
    own, got = refs[0], refs[1:n_ep]
    scales, weight, shared_down, out = refs[n_ep:]
    e = lax.axis_index("ep")
    c = lax.rem(lax.axis_index("tp"), 2)
    h = c if mine else 1 - c
    size = weight.shape[2] // (2 * n_z)
    rows = inner.shape[1]
    batch = rows // n_ep
    local, width = inner.shape[0], shared_down.shape[0]
    total = own[...]
    for k in range(1, n_ep):
        floats = got[k - 1][...].astype(F32)
        total = total + jnp.concatenate(
            [floats[(j ^ k) * batch : ((j ^ k) + 1) * batch] for j in range(n_ep)], axis=0
        )
    total = total * scales[:, 0:1]
    padded = total.shape[1] // 2
    shared = silu(total[:, :padded]) * total[:, padded:] * scales[:, 1:2]
    shared = shared[:, :width].astype(BF16)
    ratio = shared_down.shape[1] // size
    for z in range(n_z):
        lanes = lane_slice(2 * z + h, size)
        part = dot(inner[0], weight[0, :, lanes])
        for i in range(1, local):
            part = part + dot(inner[i], weight[i, :, lanes])
        out[:, z * size : (z + 1) * size] = part.astype(out.dtype)
    for z in range(n_z):
        q = 2 * z + h

        @pl.when(lax.div(q, ratio) == e)
        def _():
            lanes = slice(z * size, (z + 1) * size)
            extra = dot(shared, shared_down[:, lane_slice(lax.rem(q, ratio), size)])
            out[:, lanes] = (out[:, lanes].astype(F32) + extra).astype(out.dtype)


def merge_kernel(n_ep, keep, got, own, *sent):
    batch = own.shape[0]
    total = keep[...] + got[...].astype(F32)
    own[...] = total[:batch]
    for k in range(1, n_ep):
        sent[k - 1][...] = total[k * batch : (k + 1) * batch].astype(BF16)


def gather_kernel(n_ep, n_z, *refs):
    own, got = refs[0], refs[1:n_ep]
    hidden, base, sent, scratch = refs[n_ep], refs[n_ep + 1], refs[n_ep + 2 : -1], refs[-1]
    z = lax.div(lax.axis_index("tp"), 2)
    size = base.shape[1]
    total = own[...]
    for g in got:
        total = total + g[...].astype(F32)
    scratch[...] = total
    base[...] = hidden[...] + scratch[:, lane_slice(z, size)]
    for m in range(1, n_z):
        sent[m - 1][...] = scratch[:, lane_slice(z ^ m, size)].astype(BF16)


def finish_kernel(*refs):
    total = refs[0][...]
    for r in refs[1:-1]:
        total = total + r[...].astype(F32)
    refs[-1][...] = total.astype(BF16)


def make_body(n_ep, n_tp):
    n_z = n_tp // 2

    def ep_swap(value, k):
        return swap(value, "ep", n_ep, k)

    def z_swap(value, m):
        return swap(value, "tp", n_tp, 2 * m)

    def core_swap(value):
        return swap(value, "tp", n_tp, 1)

    def body(
        tokens, norm_gain, w_query, w_forget, w_input, w_outgate, forget_floor, head_gain,
        recurrent_state, w_output, ffn_gain, w_router, routes, expert_gate, expert_up,
        expert_down, shared_gate_w, shared_up_w, shared_down_w, branch_gate,
    ):
        batch, width = tokens.shape
        rows = n_ep * batch
        block = width // n_ep
        half = block // 2
        heads, size = recurrent_state.shape[1:3]
        channels = heads * size
        local, _, inner_width = expert_gate.shape
        shared_width = shared_gate_w.shape[1]
        slice_width = width // n_tp
        side = n_z * slice_width
        others = range(1, n_ep)

        payloads = call(
            functools.partial(prepare_kernel, n_ep),
            [((batch, block + LANES), BF16)] * n_ep,
            [VMEM, VMEM],
            (tokens, routes.T),
        )
        own_payload = payloads[0]
        payloads = [own_payload] + [ep_swap(payloads[k], k) for k in others]

        (*weights, state), token = fetch(
            (w_query, w_forget, w_input, w_outgate, recurrent_state), own_payload
        )
        inverse, router = call(
            inverse_kernel,
            [((batch, LANES), F32), ((w_router.shape[1] + 8, width), BF16)],
            [VMEM] * 3,
            (tokens, w_router.T, branch_gate[None]),
        )

        own, *sent = call(
            functools.partial(project_kernel, n_ep),
            [((batch, 4 * channels), F32)] + [((batch, 4 * channels), BF16)] * (n_ep - 1),
            [VMEM] * (n_ep + 6),
            (*payloads, norm_gain[None], *weights, token),
            flops=8 * rows * block * channels,
        )
        got = [ep_swap(sent[k - 1], k) for k in others]

        mixed, gates = call(
            functools.partial(read_kernel, n_ep),
            [((batch, channels), BF16), ((batch, 3 * channels), F32)],
            [VMEM] * (n_ep + 4),
            (own, *got, inverse, forget_floor[None], head_gain[None], state),
            [pltpu.VMEM((batch, channels), F32)],
            flops=1 << 24,
        )
        mixed_all = [mixed] + [ep_swap(mixed, k) for k in others]

        group = 8
        state_spec = pl.BlockSpec((group, heads, size, size), lambda i: (i, 0, 0, 0))
        new_state, token = pl.pallas_call(
            update_kernel,
            grid=(batch // group,),
            out_shape=[
                jax.ShapeDtypeStruct(recurrent_state.shape, F32),
                jax.ShapeDtypeStruct((8, LANES), F32),
            ],
            in_specs=[pl.BlockSpec((group, 3 * channels), lambda i: (i, 0)), state_spec],
            out_specs=[state_spec, pl.BlockSpec((8, LANES), lambda i: (0, 0))],
            cost_estimate=pl.CostEstimate(flops=1 << 24, bytes_accessed=0, transcendentals=0),
            compiler_params=pltpu.CompilerParams(vmem_limit_bytes=16 << 20),
        )(gates, state)

        give, keep = call(
            functools.partial(output_kernel, n_ep),
            [((rows, half), BF16), ((rows, half), F32)],
            [VMEM] * (n_ep + 2),
            (*mixed_all, w_output, token),
            flops=2 * rows * channels * block,
        )
        core = core_swap(give)
        (summed,) = call(add_kernel, [((rows, half), BF16)], [VMEM] * 2, (keep, core))
        along = [z_swap(summed, m) for m in range(1, n_z)]
        (gate_w, up_w, down_w), token = fetch(
            (jnp.swapaxes(expert_gate, 1, 2), jnp.swapaxes(expert_up, 1, 2), expert_down), summed
        )
        (part,) = call(
            functools.partial(hidden_kernel, n_ep, n_z),
            [((rows, half), BF16)],
            [VMEM] * (n_ep + n_z + 2),
            (*payloads, keep, core, *along, token),
        )

        pieces = [part] + [ep_swap(part, k) for k in others]
        sibling = core_swap(part)
        padded = -(-shared_width // LANES) * LANES
        shared_own, shared_sent = call(
            shared_kernel,
            [((rows, 2 * padded), F32), ((rows, 2 * padded), BF16)],
            [VMEM] * 5,
            (
                part, sibling, ffn_gain[None],
                jnp.swapaxes(shared_gate_w, 0, 1), jnp.swapaxes(shared_up_w, 0, 1),
            ),
            flops=4 * rows * block * shared_width,
        )
        siblings = [sibling] + [core_swap(pieces[k]) for k in others]
        shared_got = [ep_swap(shared_sent, k) for k in others]

        inner, scales, own_hidden = call(
            functools.partial(expert_kernel, n_ep),
            [
                ((local, rows, inner_width), BF16),
                ((rows, LANES), F32),
                ((batch, slice_width), F32),
            ],
            [VMEM] * (3 * n_ep + 4),
            (*pieces, *siblings, *payloads, ffn_gain[None], router, gate_w, up_w),
            [pltpu.VMEM((rows, width), F32), pltpu.VMEM((rows, width), BF16)],
            flops=4 * rows * width * inner_width * local,
        )

        def down(mine, dtype):
            return call(
                functools.partial(down_kernel, n_ep, n_z, mine),
                [((rows, side), dtype)],
                [VMEM] * (n_ep + 4),
                (inner, shared_own, *shared_got, scales, down_w, shared_down_w),
                flops=rows * width * inner_width * local,
            )[0]

        core = core_swap(down(False, BF16))
        keep = down(True, F32)
        own, *sent = call(
            functools.partial(merge_kernel, n_ep),
            [((batch, side), F32)] + [((batch, side), BF16)] * (n_ep - 1),
            [VMEM] * 2,
            (keep, core),
        )
        got = [ep_swap(sent[k - 1], k) for k in others]
        base, *sent = call(
            functools.partial(gather_kernel, n_ep, n_z),
            [((batch, slice_width), F32)] + [((batch, slice_width), BF16)] * (n_z - 1),
            [VMEM] * (n_ep + 1),
            (own, *got, own_hidden),
            [pltpu.VMEM((batch, side), F32)],
        )
        got = [z_swap(sent[m - 1], m) for m in range(1, n_z)]
        (layer_out,) = call(
            finish_kernel, [((batch, slice_width), BF16)], [VMEM] * n_z, (base, *got)
        )
        return layer_out, new_state

    return body


def solution(mesh):
    return jax.shard_map(
        make_body(mesh.shape["ep"], mesh.shape["tp"]),
        mesh=mesh,
        in_specs=(
            P("ep", None),
            P(),
            P("ep", "tp"),
            P("ep", "tp"),
            P("ep", "tp"),
            P("ep", "tp"),
            P("tp"),
            P("tp"),
            P("ep", "tp", None, None),
            P("tp", "ep"),
            P(),
            P(),
            P("ep", None),
            P("ep", None, "tp"),
            P("ep", None, "tp"),
            P("ep", "tp", None),
            P("ep", "tp"),
            P("ep", "tp"),
            P("tp", "ep"),
            P(),
        ),
        out_specs=(P("ep", "tp"), P("ep", "tp", None, None)),
        check_vma=False,
    )
```

```python
import functools

import jax
import jax.numpy as jnp
from jax import lax
from jax.experimental import pallas as pl
from jax.experimental.pallas import tpu as pltpu
from jax.sharding import PartitionSpec as P


NORM_EPSILON = 1e-06
ROUTED_SCALE = 2.5
LANES = 128
F32 = jnp.float32
BF16 = jnp.bfloat16
VMEM = pl.BlockSpec(memory_space=pltpu.VMEM)
HBM = pl.BlockSpec(memory_space=pltpu.HBM)


def dot(a, b):
    return jnp.dot(a, b, preferred_element_type=F32)


def dot_t(a, b):
    return lax.dot_general(a, b, (((1,), (1,)), ((), ())), preferred_element_type=F32)


def silu(x):
    return x * jax.nn.sigmoid(x)


def swap(value, axis, size, step):
    return lax.ppermute(value, axis, [(s, s ^ step) for s in range(size)])


def inverse_rms(floats):
    return lax.rsqrt(jnp.mean(floats * floats, axis=-1, keepdims=True) + NORM_EPSILON)


def lane_slice(index, size):
    return pl.ds(pl.multiple_of(index * size, LANES), size)


def call(body, outs, ins, args, scratch=(), flops=0, limit=24):
    return pl.pallas_call(
        body,
        out_shape=[jax.ShapeDtypeStruct(s, d) for s, d in outs],
        in_specs=ins,
        out_specs=[VMEM] * len(outs),
        scratch_shapes=list(scratch),
        cost_estimate=pl.CostEstimate(flops=flops, bytes_accessed=0, transcendentals=0),
        compiler_params=pltpu.CompilerParams(vmem_limit_bytes=limit << 20),
    )(*args)


def prepare_kernel(tokens, *refs):
    outs, sems = refs[:-1], refs[-1]
    e = lax.axis_index("ep")
    block = outs[0].shape[1]
    copies = [
        pltpu.make_async_copy(tokens.at[:, lane_slice(e ^ k, block)], out, sems.at[k])
        for k, out in enumerate(outs)
    ]
    for copy in copies:
        copy.start()
    for copy in copies:
        copy.wait()


def route_mask(routes_t):
    batch = routes_t.shape[1]
    names = lax.broadcasted_iota(jnp.int32, (LANES, batch), 0)
    hit = names == routes_t[0:1, :]
    for j in range(1, routes_t.shape[0]):
        hit = hit | (names == routes_t[j : j + 1, :])
    eye = lax.broadcasted_iota(jnp.int32, (batch, batch), 0) == lax.broadcasted_iota(
        jnp.int32, (batch, batch), 1
    )
    return dot_t(jnp.where(eye, 1.0, 0.0).astype(BF16), jnp.where(hit, 1.0, 0.0).astype(BF16))


def fetch_kernel(arrays, *refs):
    sources, copied, token, sems = refs[:arrays], refs[-arrays - 2 : -2], refs[-2], refs[-1]
    copies = []
    for source, target in zip(sources, copied, strict=True):
        rows = target.shape[0]
        whole = 1 if target.ndim == 2 else rows
        parts = 4 if rows % (32 if target.ndim == 2 else 4) == 0 else whole
        step = rows // parts
        for p in range(parts):
            span = pl.ds(p * step, step)
            copies.append(
                pltpu.make_async_copy(source.at[span], target.at[span], sems.at[len(copies)])
            )
    for copy in copies:
        copy.start()
    for copy in copies:
        copy.wait()
    token[...] = jnp.zeros_like(token)


def fetch(arrays, after):
    arrays = [pltpu.with_memory_space_constraint(a, pltpu.HBM) for a in arrays]
    *copied, token = call(
        functools.partial(fetch_kernel, len(arrays)),
        [(a.shape, a.dtype) for a in arrays] + [((8, LANES), F32)],
        [HBM] * len(arrays) + [VMEM],
        (*arrays, after),
        [pltpu.SemaphoreType.DMA((24 * len(arrays),))],
        flops=1 << 26,
        limit=1,
    )
    return copied, token


def inverse_kernel(tokens, router_t, branch, out, router):
    out[...] = jnp.broadcast_to(inverse_rms(tokens[...].astype(F32)), out.shape)
    extra = jnp.broadcast_to(branch[...].astype(F32), (8, branch.shape[1]))
    router[...] = jnp.concatenate([router_t[...].astype(F32), extra], axis=0).astype(BF16)


def project_kernel(n_ep, *refs):
    payloads, gain, weights = refs[:n_ep], refs[n_ep], refs[n_ep + 1 : n_ep + 5]
    own, sent = refs[n_ep + 6], refs[n_ep + 7 :]
    batch = own.shape[0]
    block, channels = weights[0].shape
    row = gain[:, lane_slice(lax.axis_index("ep"), block)]
    scaled = jnp.concatenate([p[...].astype(F32) for p in payloads], axis=0) * row
    scaled = scaled.astype(BF16)
    for i, weight in enumerate(weights):
        part = dot(scaled, weight[...])
        lanes = slice(i * channels, (i + 1) * channels)
        own[:, lanes] = part[:batch]
        for k in range(1, n_ep):
            sent[k - 1][:, lanes] = part[k * batch : (k + 1) * batch].astype(BF16)


def columns_of(value):
    rows, lanes = value.shape
    return jnp.concatenate([value, jnp.zeros((LANES - rows, lanes), F32)], axis=0).T


def read_kernel(n_ep, *refs):
    own, got = refs[0], refs[1:n_ep]
    inverse, floor, head_gain, state, routes_t = refs[n_ep : n_ep + 5]
    mixed, gates, scratch = refs[n_ep + 6 :]
    batch, heads, size = state.shape[:3]
    channels = heads * size
    total = own[...]
    for g in got:
        total = total + g[...].astype(F32)
    total = total * inverse[:, 0:1]
    query, forget_pre, value, out_gate = (
        total[:, i * channels : (i + 1) * channels] for i in range(4)
    )
    low = floor[...]
    forget = low + (1.0 - low) * jax.nn.sigmoid(forget_pre)
    key = (1.0 - low) * jax.nn.sigmoid(-forget_pre)
    gates[:, :channels] = forget
    gates[:, channels : 2 * channels] = key
    gates[:, 2 * channels :] = value
    active = silu(query)
    weight = columns_of(active * forget)
    for b in range(batch):
        for h in range(heads):
            column = weight[h * size : (h + 1) * size, b : b + 1]
            scratch[b : b + 1, h * size : (h + 1) * size] = jnp.sum(
                column * state[b, h], axis=0, keepdims=True
            )
    mixed[:, channels:] = route_mask(routes_t[...]).astype(BF16)
    scale = head_gain[...] * silu(out_gate)
    for h in range(heads):
        lanes = slice(h * size, (h + 1) * size)
        read = scratch[:, lanes] + value[:, lanes] * jnp.sum(
            active[:, lanes] * key[:, lanes], axis=-1, keepdims=True
        )
        mixed[:, lanes] = (read * inverse_rms(read) * scale[:, lanes]).astype(BF16)


def update_kernel(group, gates, state, out, token, buffer, sems):
    batch, heads, size = state.shape[:3]
    channels = heads * size
    forget = columns_of(gates[:, :channels])
    key = columns_of(gates[:, channels : 2 * channels])
    copies = []
    for b in range(batch):
        for h in range(heads):
            rows = slice(h * size, (h + 1) * size)
            value = gates[b : b + 1, 2 * channels + h * size : 2 * channels + (h + 1) * size]
            buffer[b, h] = forget[rows, b : b + 1] * state[b, h] + key[rows, b : b + 1] * value
        if (b + 1) % group == 0:
            span = pl.ds(b + 1 - group, group)
            copies.append(
                pltpu.make_async_copy(buffer.at[span], out.at[span], sems.at[len(copies)])
            )
            copies[-1].start()
    for copy in copies:
        copy.wait()
    token[...] = jnp.zeros_like(token)


def output_kernel(n_ep, *refs):
    mixed, weight, give, keep = refs[:n_ep], refs[n_ep], refs[-2], refs[-1]
    c = lax.rem(lax.axis_index("tp"), 2)
    half = keep.shape[1]
    rows = jnp.concatenate([m[...].astype(F32) for m in mixed], axis=0).astype(BF16)
    rows = rows[:, : weight.shape[0]]
    give[...] = dot(rows, weight[:, lane_slice(1 - c, half)]).astype(BF16)
    keep[...] = dot(rows, weight[:, lane_slice(c, half)])


def add_kernel(keep, got, out):
    out[...] = (keep[...] + got[...].astype(F32)).astype(BF16)


def hidden_kernel(n_ep, *refs):
    payloads, keep, core, others = refs[:n_ep], refs[n_ep], refs[n_ep + 1], refs[n_ep + 2 : -2]
    out = refs[-1]
    c = lax.rem(lax.axis_index("tp"), 2)
    half = keep.shape[1]
    total = jnp.concatenate([p[:, lane_slice(c, half)].astype(F32) for p in payloads], axis=0)
    mixed = keep[...] + core[...].astype(F32)
    for other in others:
        mixed = mixed + other[...].astype(F32)
    out[...] = (total + mixed).astype(BF16)


def shared_kernel(mine, other, gain, gate_t, up_t, own, sent):
    c = lax.rem(lax.axis_index("tp"), 2)
    e = lax.axis_index("ep")
    half = mine.shape[1]
    inner, padded = gate_t.shape[0], own.shape[1] // 2
    own[...] = jnp.zeros_like(own)
    total = [None, None]
    for piece, h in ((mine, c), (other, 1 - c)):
        row = gain[:, lane_slice(2 * e + h, half)]
        scaled = (piece[...].astype(F32) * row).astype(BF16)
        for i, weight in enumerate((gate_t, up_t)):
            part = dot_t(scaled, weight[:, lane_slice(h, half)])
            total[i] = part if total[i] is None else total[i] + part
    for i in range(2):
        own[:, i * padded : i * padded + inner] = total[i]
    sent[...] = own[...].astype(BF16)


def expert_kernel(n_ep, *refs):
    pieces, others, payloads = refs[:n_ep], refs[n_ep : 2 * n_ep], refs[2 * n_ep : 3 * n_ep]
    gain, router, gate_w, up_w, down = refs[3 * n_ep : 3 * n_ep + 5]
    inner, scales, own_hidden, down_out, x_ref, n_ref, sems = refs[3 * n_ep + 5 :]
    local = inner.shape[0]
    fetches = [
        pltpu.make_async_copy(down.at[i], down_out.at[i], sems.at[i]) for i in range(local)
    ]
    for copy in fetches:
        copy.start()
    e = lax.axis_index("ep")
    t = lax.axis_index("tp")
    c = lax.rem(t, 2)
    rows, half = pieces[0].shape
    batch = rows // n_ep
    squares = jnp.zeros((rows, half), F32)
    for k in range(n_ep):
        for source, h in ((pieces[k], c), (others[k], 1 - c)):
            floats = source[...].astype(F32)
            floats = jnp.concatenate(
                [floats[(j ^ k) * batch : ((j ^ k) + 1) * batch] for j in range(n_ep)], axis=0
            )
            squares = squares + floats * floats
            x_ref[:, lane_slice(2 * (e ^ k) + h, half)] = floats
    width = x_ref.shape[1]
    inv = lax.rsqrt(jnp.sum(squares, axis=-1, keepdims=True) / width + NORM_EPSILON)
    own_hidden[...] = x_ref[:batch, lane_slice(t, own_hidden.shape[1])]
    n_ref[...] = (x_ref[...] * inv * gain[...]).astype(BF16)
    scores = jax.nn.sigmoid(dot_t(n_ref[...], router[...]))
    experts = router.shape[0] - 8
    lane = lax.broadcasted_iota(jnp.int32, scores.shape, 1)
    start = payloads[0].shape[1] - LANES
    mask = jnp.concatenate([p[:, start:].astype(F32) for p in payloads], axis=0)
    chosen = jnp.where(mask[:, : router.shape[0]] > 0.5, scores, 0.0)
    weights = chosen / jnp.sum(chosen, axis=1, keepdims=True) * ROUTED_SCALE
    branch = jnp.sum(jnp.where(lane == experts, scores, 0.0), axis=1, keepdims=True)
    spread = lax.broadcasted_iota(jnp.int32, scales.shape, 1)
    scales[...] = jnp.where(spread == 0, inv, branch)
    for i in range(local):
        combine = jnp.sum(jnp.where(lane == e * local + i, weights, 0.0), axis=1, keepdims=True)
        gate = dot_t(n_ref[...], gate_w[i])
        up = dot_t(n_ref[...], up_w[i])
        inner[i] = (silu(gate) * up * combine).astype(BF16)
    for copy in fetches:
        copy.wait()


def shared_activation(n_ep, shape, own, *refs):
    got, scales = refs[:-1], refs[-1]
    rows, width = shape
    batch = rows // n_ep
    total = own[...]
    for k in range(1, n_ep):
        floats = got[k - 1][...].astype(F32)
        total = total + jnp.concatenate(
            [floats[(j ^ k) * batch : ((j ^ k) + 1) * batch] for j in range(n_ep)], axis=0
        )
    total = total * scales[:, 0:1]
    padded = total.shape[1] // 2
    shared = silu(total[:, :padded]) * total[:, padded:] * scales[:, 1:2]
    return shared[:, :width].astype(BF16)


def down_kernel(n_ep, n_z, mine, inner, *refs):
    if mine:
        shared, weight, shared_down, out = refs
    else:
        *refs, weight, shared_down, out, shared = refs
        shared[...] = shared_activation(n_ep, shared.shape, *refs)
    e = lax.axis_index("ep")
    c = lax.rem(lax.axis_index("tp"), 2)
    h = c if mine else 1 - c
    size = weight.shape[2] // (2 * n_z)
    local = inner.shape[0]
    ratio = shared_down.shape[1] // size
    for z in range(n_z):
        lanes = lane_slice(2 * z + h, size)
        part = dot(inner[0], weight[0, :, lanes])
        for i in range(1, local):
            part = part + dot(inner[i], weight[i, :, lanes])
        out[:, z * size : (z + 1) * size] = part.astype(out.dtype)
    for z in range(n_z):
        q = 2 * z + h

        @pl.when(lax.div(q, ratio) == e)
        def _():
            lanes = slice(z * size, (z + 1) * size)
            extra = dot(shared[...], shared_down[:, lane_slice(lax.rem(q, ratio), size)])
            out[:, lanes] = (out[:, lanes].astype(F32) + extra).astype(out.dtype)


def merge_kernel(n_ep, keep, got, own, *sent):
    batch = own.shape[0]
    total = keep[...] + got[...].astype(F32)
    own[...] = total[:batch]
    for k in range(1, n_ep):
        sent[k - 1][...] = total[k * batch : (k + 1) * batch].astype(BF16)


def gather_kernel(n_ep, n_z, *refs):
    own, got = refs[0], refs[1:n_ep]
    hidden, base, sent, scratch = refs[n_ep], refs[n_ep + 1], refs[n_ep + 2 : -1], refs[-1]
    z = lax.div(lax.axis_index("tp"), 2)
    size = base.shape[1]
    total = own[...]
    for g in got:
        total = total + g[...].astype(F32)
    scratch[...] = total
    base[...] = hidden[...] + scratch[:, lane_slice(z, size)]
    for m in range(1, n_z):
        sent[m - 1][...] = scratch[:, lane_slice(z ^ m, size)].astype(BF16)


def finish_kernel(*refs):
    total = refs[0][...]
    for r in refs[1:-1]:
        total = total + r[...].astype(F32)
    refs[-1][...] = total.astype(BF16)


def make_body(n_ep, n_tp):
    n_z = n_tp // 2

    def ep_swap(value, k):
        return swap(value, "ep", n_ep, k)

    def z_swap(value, m):
        return swap(value, "tp", n_tp, 2 * m)

    def core_swap(value):
        return swap(value, "tp", n_tp, 1)

    def body(
        tokens, norm_gain, w_query, w_forget, w_input, w_outgate, forget_floor, head_gain,
        recurrent_state, w_output, ffn_gain, w_router, routes, expert_gate, expert_up,
        expert_down, shared_gate_w, shared_up_w, shared_down_w, branch_gate,
    ):
        batch, width = tokens.shape
        rows = n_ep * batch
        block = width // n_ep
        half = block // 2
        heads, size = recurrent_state.shape[1:3]
        channels = heads * size
        local, _, inner_width = expert_gate.shape
        shared_width = shared_gate_w.shape[1]
        slice_width = width // n_tp
        side = n_z * slice_width
        others = range(1, n_ep)

        payloads = call(
            prepare_kernel,
            [((batch, block), BF16)] * n_ep,
            [HBM],
            (pltpu.with_memory_space_constraint(tokens, pltpu.HBM),),
            [pltpu.SemaphoreType.DMA((n_ep,))],
        )
        own_payload = payloads[0]
        payloads = [own_payload] + [ep_swap(payloads[k], k) for k in others]

        (*weights, gain), token = fetch(
            (w_query, w_forget, w_input, w_outgate, norm_gain[None]), own_payload
        )
        own, *sent = call(
            functools.partial(project_kernel, n_ep),
            [((batch, 4 * channels), F32)] + [((batch, 4 * channels), BF16)] * (n_ep - 1),
            [VMEM] * (n_ep + 6),
            (*payloads, gain, *weights, token),
            flops=8 * rows * block * channels,
        )
        got = [ep_swap(sent[k - 1], k) for k in others]
        (state, full, router_t), token = fetch((recurrent_state, tokens, w_router.T), own)
        inverse, router = call(
            inverse_kernel,
            [((batch, LANES), F32), ((w_router.shape[1] + 8, width), BF16)],
            [VMEM] * 3,
            (full, router_t, branch_gate[None]),
        )


        mixed, gates = call(
            functools.partial(read_kernel, n_ep),
            [((batch, channels + LANES), BF16), ((batch, 3 * channels), F32)],
            [VMEM] * (n_ep + 6),
            (own, *got, inverse, forget_floor[None], head_gain[None], state, routes.T, token),
            [pltpu.VMEM((batch, channels), F32)],
            flops=1 << 24,
        )
        mixed_all = [mixed] + [ep_swap(mixed, k) for k in others]

        group = 4
        new_state, token = pl.pallas_call(
            functools.partial(update_kernel, group),
            out_shape=[
                jax.ShapeDtypeStruct(recurrent_state.shape, F32),
                jax.ShapeDtypeStruct((8, LANES), F32),
            ],
            in_specs=[VMEM] * 2,
            out_specs=[HBM, VMEM],
            scratch_shapes=[
                pltpu.VMEM(recurrent_state.shape, F32),
                pltpu.SemaphoreType.DMA((batch // group,)),
            ],
            cost_estimate=pl.CostEstimate(flops=1 << 26, bytes_accessed=0, transcendentals=0),
            compiler_params=pltpu.CompilerParams(vmem_limit_bytes=16 << 20),
        )(gates, state)

        give, keep = call(
            functools.partial(output_kernel, n_ep),
            [((rows, half), BF16), ((rows, half), F32)],
            [VMEM] * (n_ep + 2),
            (*mixed_all, w_output, token),
            flops=2 * rows * channels * block,
        )
        core = core_swap(give)
        (summed,) = call(add_kernel, [((rows, half), BF16)], [VMEM] * 2, (keep, core))
        along = [z_swap(summed, m) for m in range(1, n_z)]
        (gate_w, up_w), token = fetch(
            (jnp.swapaxes(expert_gate, 1, 2), jnp.swapaxes(expert_up, 1, 2)), summed
        )
        (part,) = call(
            functools.partial(hidden_kernel, n_ep),
            [((rows, half), BF16)],
            [VMEM] * (n_ep + n_z + 2),
            (*payloads, keep, core, *along, token),
        )

        pieces = [part] + [ep_swap(part, k) for k in others]
        sibling = core_swap(part)
        padded = -(-shared_width // LANES) * LANES
        shared_own, shared_sent = call(
            shared_kernel,
            [((rows, 2 * padded), F32), ((rows, 2 * padded), BF16)],
            [VMEM] * 5,
            (
                part, sibling, ffn_gain[None],
                jnp.swapaxes(shared_gate_w, 0, 1), jnp.swapaxes(shared_up_w, 0, 1),
            ),
            flops=4 * rows * block * shared_width,
        )
        siblings = [sibling] + [core_swap(pieces[k]) for k in others]
        shared_got = [ep_swap(shared_sent, k) for k in others]

        inner, scales, own_hidden, down_w = call(
            functools.partial(expert_kernel, n_ep),
            [
                ((local, rows, inner_width), BF16),
                ((rows, LANES), F32),
                ((batch, slice_width), F32),
                (expert_down.shape, BF16),
            ],
            [VMEM] * (3 * n_ep + 4) + [HBM],
            (
                *pieces, *siblings, *mixed_all, ffn_gain[None], router, gate_w, up_w,
                pltpu.with_memory_space_constraint(expert_down, pltpu.HBM),
            ),
            [
                pltpu.VMEM((rows, width), F32),
                pltpu.VMEM((rows, width), BF16),
                pltpu.SemaphoreType.DMA((local,)),
            ],
            flops=4 * rows * width * inner_width * local,
        )

        give, shared = call(
            functools.partial(down_kernel, n_ep, n_z, False),
            [((rows, side), BF16), ((rows, shared_width), BF16)],
            [VMEM] * (n_ep + 4),
            (inner, shared_own, *shared_got, scales, down_w, shared_down_w),
            flops=rows * width * inner_width * local,
        )
        core = core_swap(give)
        (keep,) = call(
            functools.partial(down_kernel, n_ep, n_z, True),
            [((rows, side), F32)],
            [VMEM] * 4,
            (inner, shared, down_w, shared_down_w),
            flops=rows * width * inner_width * local,
        )
        own, *sent = call(
            functools.partial(merge_kernel, n_ep),
            [((batch, side), F32)] + [((batch, side), BF16)] * (n_ep - 1),
            [VMEM] * 2,
            (keep, core),
        )
        got = [ep_swap(sent[k - 1], k) for k in others]
        base, *sent = call(
            functools.partial(gather_kernel, n_ep, n_z),
            [((batch, slice_width), F32)] + [((batch, slice_width), BF16)] * (n_z - 1),
            [VMEM] * (n_ep + 1),
            (own, *got, own_hidden),
            [pltpu.VMEM((batch, side), F32)],
        )
        got = [z_swap(sent[m - 1], m) for m in range(1, n_z)]
        (layer_out,) = call(
            finish_kernel, [((batch, slice_width), BF16)], [VMEM] * n_z, (base, *got)
        )
        return layer_out, new_state

    return body


def solution(mesh):
    body = make_body(mesh.shape["ep"], mesh.shape["tp"])

    return jax.shard_map(
        body,
        mesh=mesh,
        in_specs=(
            P("ep", None),
            P(),
            P("ep", "tp"),
            P("ep", "tp"),
            P("ep", "tp"),
            P("ep", "tp"),
            P("tp"),
            P("tp"),
            P("ep", "tp", None, None),
            P("tp", "ep"),
            P(),
            P(),
            P("ep", None),
            P("ep", None, "tp"),
            P("ep", None, "tp"),
            P("ep", "tp", None),
            P("ep", "tp"),
            P("ep", "tp"),
            P("tp", "ep"),
            P(),
        ),
        out_specs=(P("ep", "tp"), P("ep", "tp", None, None)),
        check_vma=False,
    )
```

```python
import functools

import jax
import jax.numpy as jnp
from jax import lax
from jax.experimental import pallas as pl
from jax.experimental.pallas import tpu as pltpu
from jax.sharding import PartitionSpec as P


NORM_EPSILON = 1e-06
ROUTED_SCALE = 2.5
LANES = 128
F32 = jnp.float32
BF16 = jnp.bfloat16
VMEM = pl.BlockSpec(memory_space=pltpu.VMEM)
HBM = pl.BlockSpec(memory_space=pltpu.HBM)


def dot(a, b):
    return jnp.dot(a, b, preferred_element_type=F32)


def dot_t(a, b):
    return lax.dot_general(a, b, (((1,), (1,)), ((), ())), preferred_element_type=F32)


def silu(x):
    return x * jax.nn.sigmoid(x)


def swap(value, axis, size, step):
    return lax.ppermute(value, axis, [(s, s ^ step) for s in range(size)])


def inverse_rms(floats):
    return lax.rsqrt(jnp.mean(floats * floats, axis=-1, keepdims=True) + NORM_EPSILON)


def lane_slice(index, size):
    return pl.ds(pl.multiple_of(index * size, LANES), size)


def half_index():
    t = lax.axis_index("tp")
    return lax.rem(t + lax.div(t, 2) + lax.axis_index("ep"), 2)


def call(body, outs, ins, args, scratch=(), flops=0, limit=24):
    return pl.pallas_call(
        body,
        out_shape=[jax.ShapeDtypeStruct(s, d) for s, d in outs],
        in_specs=ins,
        out_specs=[VMEM] * len(outs),
        scratch_shapes=list(scratch),
        cost_estimate=pl.CostEstimate(flops=flops, bytes_accessed=0, transcendentals=0),
        compiler_params=pltpu.CompilerParams(vmem_limit_bytes=limit << 20),
    )(*args)


def prepare_kernel(tokens, *refs):
    outs, sems = refs[:-1], refs[-1]
    e = lax.axis_index("ep")
    block = outs[0].shape[1]
    copies = [
        pltpu.make_async_copy(tokens.at[:, lane_slice(e ^ k, block)], out, sems.at[k])
        for k, out in enumerate(outs)
    ]
    for copy in copies:
        copy.start()
    for copy in copies:
        copy.wait()


def route_mask(routes_t):
    batch = routes_t.shape[1]
    names = lax.broadcasted_iota(jnp.int32, (LANES, batch), 0)
    hit = names == routes_t[0:1, :]
    for j in range(1, routes_t.shape[0]):
        hit = hit | (names == routes_t[j : j + 1, :])
    eye = lax.broadcasted_iota(jnp.int32, (batch, batch), 0) == lax.broadcasted_iota(
        jnp.int32, (batch, batch), 1
    )
    return dot_t(jnp.where(eye, 1.0, 0.0).astype(BF16), jnp.where(hit, 1.0, 0.0).astype(BF16))


def fetch_kernel(arrays, *refs):
    sources, copied, token, sems = refs[:arrays], refs[-arrays - 2 : -2], refs[-2], refs[-1]
    copies = []
    for source, target in zip(sources, copied, strict=True):
        rows = target.shape[0]
        whole = 1 if target.ndim == 2 else rows
        parts = 4 if rows % (32 if target.ndim == 2 else 4) == 0 else whole
        step = rows // parts
        for p in range(parts):
            span = pl.ds(p * step, step)
            copies.append(
                pltpu.make_async_copy(source.at[span], target.at[span], sems.at[len(copies)])
            )
    for copy in copies:
        copy.start()
    for copy in copies:
        copy.wait()
    token[...] = jnp.zeros_like(token)


def fetch(arrays, after):
    arrays = [pltpu.with_memory_space_constraint(a, pltpu.HBM) for a in arrays]
    *copied, token = call(
        functools.partial(fetch_kernel, len(arrays)),
        [(a.shape, a.dtype) for a in arrays] + [((8, LANES), F32)],
        [HBM] * len(arrays) + [VMEM],
        (*arrays, after),
        [pltpu.SemaphoreType.DMA((24 * len(arrays),))],
        flops=1 << 26,
        limit=1,
    )
    return copied, token


def inverse_kernel(tokens, router_t, branch, out, router):
    out[...] = jnp.broadcast_to(inverse_rms(tokens[...].astype(F32)), out.shape)
    extra = jnp.broadcast_to(branch[...].astype(F32), (8, branch.shape[1]))
    router[...] = jnp.concatenate([router_t[...].astype(F32), extra], axis=0).astype(BF16)


def project_kernel(n_ep, *refs):
    payloads, gain, weights = refs[:n_ep], refs[n_ep], refs[n_ep + 1 : n_ep + 5]
    own, sent = refs[n_ep + 6], refs[n_ep + 7 :]
    batch = own.shape[0]
    block, channels = weights[0].shape
    row = gain[:, lane_slice(lax.axis_index("ep"), block)]
    scaled = jnp.concatenate([p[...].astype(F32) for p in payloads], axis=0) * row
    scaled = scaled.astype(BF16)
    for i, weight in enumerate(weights):
        part = dot(scaled, weight[...])
        lanes = slice(i * channels, (i + 1) * channels)
        own[:, lanes] = part[:batch]
        for k in range(1, n_ep):
            sent[k - 1][:, lanes] = part[k * batch : (k + 1) * batch].astype(BF16)


def columns_of(value):
    rows, lanes = value.shape
    return jnp.concatenate([value, jnp.zeros((LANES - rows, lanes), F32)], axis=0).T


def read_kernel(n_ep, *refs):
    own, got = refs[0], refs[1:n_ep]
    inverse, floor, head_gain, state, routes_t = refs[n_ep : n_ep + 5]
    mixed, gates, scratch = refs[n_ep + 6 :]
    batch, heads, size = state.shape[:3]
    channels = heads * size
    total = own[...]
    for g in got:
        total = total + g[...].astype(F32)
    total = total * inverse[:, 0:1]
    query, forget_pre, value, out_gate = (
        total[:, i * channels : (i + 1) * channels] for i in range(4)
    )
    low = floor[...]
    forget = low + (1.0 - low) * jax.nn.sigmoid(forget_pre)
    key = (1.0 - low) * jax.nn.sigmoid(-forget_pre)
    gates[:, :channels] = forget
    gates[:, channels : 2 * channels] = key
    gates[:, 2 * channels :] = value
    active = silu(query)
    weight = columns_of(active * forget)
    for b in range(batch):
        for h in range(heads):
            column = weight[h * size : (h + 1) * size, b : b + 1]
            scratch[b : b + 1, h * size : (h + 1) * size] = jnp.sum(
                column * state[b, h], axis=0, keepdims=True
            )
    mixed[:, channels:] = route_mask(routes_t[...]).astype(BF16)
    scale = head_gain[...] * silu(out_gate)
    for h in range(heads):
        lanes = slice(h * size, (h + 1) * size)
        read = scratch[:, lanes] + value[:, lanes] * jnp.sum(
            active[:, lanes] * key[:, lanes], axis=-1, keepdims=True
        )
        mixed[:, lanes] = (read * inverse_rms(read) * scale[:, lanes]).astype(BF16)


def update_kernel(group, gates, state, out, token, buffer, sems):
    batch, heads, size = state.shape[:3]
    channels = heads * size
    forget = columns_of(gates[:, :channels])
    key = columns_of(gates[:, channels : 2 * channels])
    copies = []
    for b in range(batch):
        for h in range(heads):
            rows = slice(h * size, (h + 1) * size)
            value = gates[b : b + 1, 2 * channels + h * size : 2 * channels + (h + 1) * size]
            buffer[b, h] = forget[rows, b : b + 1] * state[b, h] + key[rows, b : b + 1] * value
        if (b + 1) % group == 0:
            span = pl.ds(b + 1 - group, group)
            copies.append(
                pltpu.make_async_copy(buffer.at[span], out.at[span], sems.at[len(copies)])
            )
            copies[-1].start()
    for copy in copies:
        copy.wait()
    token[...] = jnp.zeros_like(token)


def output_kernel(n_ep, *refs):
    mixed, weight, give, keep = refs[:n_ep], refs[n_ep], refs[-2], refs[-1]
    c = half_index()
    half = keep.shape[1]
    rows = jnp.concatenate([m[...].astype(F32) for m in mixed], axis=0).astype(BF16)
    rows = rows[:, : weight.shape[0]]
    give[...] = dot(rows, weight[:, lane_slice(1 - c, half)]).astype(BF16)
    keep[...] = dot(rows, weight[:, lane_slice(c, half)])


def add_kernel(keep, got, out):
    out[...] = (keep[...] + got[...].astype(F32)).astype(BF16)


def hidden_kernel(n_ep, *refs):
    payloads, keep, core, others = refs[:n_ep], refs[n_ep], refs[n_ep + 1], refs[n_ep + 2 : -2]
    out = refs[-1]
    c = half_index()
    half = keep.shape[1]
    total = jnp.concatenate([p[:, lane_slice(c, half)].astype(F32) for p in payloads], axis=0)
    mixed = keep[...] + core[...].astype(F32)
    for other in others:
        mixed = mixed + other[...].astype(F32)
    out[...] = (total + mixed).astype(BF16)


def shared_kernel(mine, other, gain, gate_t, up_t, own, sent):
    c = half_index()
    e = lax.axis_index("ep")
    half = mine.shape[1]
    inner, padded = gate_t.shape[0], own.shape[1] // 2
    own[...] = jnp.zeros_like(own)
    total = [None, None]
    for piece, h in ((mine, c), (other, 1 - c)):
        row = gain[:, lane_slice(2 * e + h, half)]
        scaled = (piece[...].astype(F32) * row).astype(BF16)
        for i, weight in enumerate((gate_t, up_t)):
            part = dot_t(scaled, weight[:, lane_slice(h, half)])
            total[i] = part if total[i] is None else total[i] + part
    for i in range(2):
        own[:, i * padded : i * padded + inner] = total[i]
    sent[...] = own[...].astype(BF16)


def expert_kernel(n_ep, *refs):
    pieces, others, payloads = refs[:n_ep], refs[n_ep : 2 * n_ep], refs[2 * n_ep : 3 * n_ep]
    gain, router, gate_w, up_w, down = refs[3 * n_ep : 3 * n_ep + 5]
    inner, scales, own_hidden, down_out, x_ref, n_ref, sems = refs[3 * n_ep + 5 :]
    local, inner_width = gate_w.shape[:2]
    spans = [slice(i * inner_width, (i + 1) * inner_width) for i in range(local)]
    fetches = [
        pltpu.make_async_copy(down.at[i], down_out.at[spans[i]], sems.at[i])
        for i in range(local)
    ]
    for copy in fetches:
        copy.start()
    e = lax.axis_index("ep")
    t = lax.axis_index("tp")
    c = half_index()
    rows, half = pieces[0].shape
    batch = rows // n_ep
    squares = jnp.zeros((rows, half), F32)
    for k in range(n_ep):
        for source, h in ((pieces[k], c), (others[k], 1 - c)):
            floats = source[...].astype(F32)
            floats = jnp.concatenate(
                [floats[(j ^ k) * batch : ((j ^ k) + 1) * batch] for j in range(n_ep)], axis=0
            )
            squares = squares + floats * floats
            x_ref[:, lane_slice(2 * (e ^ k) + h, half)] = floats
    width = x_ref.shape[1]
    inv = lax.rsqrt(jnp.sum(squares, axis=-1, keepdims=True) / width + NORM_EPSILON)
    own_hidden[...] = x_ref[:batch, lane_slice(t, own_hidden.shape[1])]
    n_ref[...] = (x_ref[...] * inv * gain[...]).astype(BF16)
    scores = jax.nn.sigmoid(dot_t(n_ref[...], router[...]))
    experts = router.shape[0] - 8
    lane = lax.broadcasted_iota(jnp.int32, scores.shape, 1)
    start = payloads[0].shape[1] - LANES
    mask = jnp.concatenate([p[:, start:].astype(F32) for p in payloads], axis=0)
    chosen = jnp.where(mask[:, : router.shape[0]] > 0.5, scores, 0.0)
    weights = chosen / jnp.sum(chosen, axis=1, keepdims=True) * ROUTED_SCALE
    branch = jnp.sum(jnp.where(lane == experts, scores, 0.0), axis=1, keepdims=True)
    spread = lax.broadcasted_iota(jnp.int32, scales.shape, 1)
    scales[...] = jnp.where(spread == 0, inv, branch)
    for i in range(local):
        combine = jnp.sum(jnp.where(lane == e * local + i, weights, 0.0), axis=1, keepdims=True)
        gate = dot_t(n_ref[...], gate_w[i])
        up = dot_t(n_ref[...], up_w[i])
        inner[:, spans[i]] = (silu(gate) * up * combine).astype(BF16)
    for copy in fetches:
        copy.wait()


def shared_activation(n_ep, shape, own, *refs):
    got, scales = refs[:-1], refs[-1]
    rows, width = shape
    batch = rows // n_ep
    total = own[...]
    for k in range(1, n_ep):
        floats = got[k - 1][...].astype(F32)
        total = total + jnp.concatenate(
            [floats[(j ^ k) * batch : ((j ^ k) + 1) * batch] for j in range(n_ep)], axis=0
        )
    total = total * scales[:, 0:1]
    padded = total.shape[1] // 2
    shared = silu(total[:, :padded]) * total[:, padded:] * scales[:, 1:2]
    return shared[:, :width].astype(BF16)


def down_kernel(n_ep, n_z, mine, inner, *refs):
    if mine:
        shared, weight, shared_down, out = refs
    else:
        *refs, weight, shared_down, out, shared = refs
        shared[...] = shared_activation(n_ep, shared.shape, *refs)
    e = lax.axis_index("ep")
    c = lax.rem(lax.axis_index("tp"), 2)
    h = c if mine else 1 - c
    size = weight.shape[1] // (2 * n_z)
    ratio = shared_down.shape[1] // size
    for z in range(n_z):
        lanes = lane_slice(2 * z + h, size)
        part = dot(inner[...], weight[:, lanes])
        out[:, z * size : (z + 1) * size] = part.astype(out.dtype)
    for z in range(n_z):
        q = 2 * z + h

        @pl.when(lax.div(q, ratio) == e)
        def _():
            lanes = slice(z * size, (z + 1) * size)
            extra = dot(shared[...], shared_down[:, lane_slice(lax.rem(q, ratio), size)])
            out[:, lanes] = (out[:, lanes].astype(F32) + extra).astype(out.dtype)


def merge_kernel(n_ep, keep, got, own, *sent):
    batch = own.shape[0]
    total = keep[...] + got[...].astype(F32)
    own[...] = total[:batch]
    for k in range(1, n_ep):
        sent[k - 1][...] = total[k * batch : (k + 1) * batch].astype(BF16)


def gather_kernel(n_ep, n_z, *refs):
    own, got = refs[0], refs[1:n_ep]
    hidden, base, sent, scratch = refs[n_ep], refs[n_ep + 1], refs[n_ep + 2 : -1], refs[-1]
    z = lax.div(lax.axis_index("tp"), 2)
    size = base.shape[1]
    total = own[...]
    for g in got:
        total = total + g[...].astype(F32)
    scratch[...] = total
    base[...] = hidden[...] + scratch[:, lane_slice(z, size)]
    for m in range(1, n_z):
        sent[m - 1][...] = scratch[:, lane_slice(z ^ m, size)].astype(BF16)


def finish_kernel(*refs):
    total = refs[0][...]
    for r in refs[1:-1]:
        total = total + r[...].astype(F32)
    refs[-1][...] = total.astype(BF16)


def make_body(n_ep, n_tp):
    n_z = n_tp // 2

    def ep_swap(value, k):
        return swap(value, "ep", n_ep, k)

    def cross_swap(value, k, flip):
        pairs = [
            (e * n_tp + t, (e ^ k) * n_tp + (t ^ flip)) for e in range(n_ep) for t in range(n_tp)
        ]
        return lax.ppermute(value, ("ep", "tp"), pairs)

    def z_swap(value, m, flip=0):
        return swap(value, "tp", n_tp, 2 * m | flip)

    def core_swap(value):
        return swap(value, "tp", n_tp, 1)

    def body(
        tokens, norm_gain, w_query, w_forget, w_input, w_outgate, forget_floor, head_gain,
        recurrent_state, w_output, ffn_gain, w_router, routes, expert_gate, expert_up,
        expert_down, shared_gate_w, shared_up_w, shared_down_w, branch_gate,
    ):
        batch, width = tokens.shape
        rows = n_ep * batch
        block = width // n_ep
        half = block // 2
        heads, size = recurrent_state.shape[1:3]
        channels = heads * size
        local, _, inner_width = expert_gate.shape
        shared_width = shared_gate_w.shape[1]
        slice_width = width // n_tp
        side = n_z * slice_width
        others = range(1, n_ep)

        payloads = call(
            prepare_kernel,
            [((batch, block), BF16)] * n_ep,
            [HBM],
            (pltpu.with_memory_space_constraint(tokens, pltpu.HBM),),
            [pltpu.SemaphoreType.DMA((n_ep,))],
        )
        own_payload = payloads[0]
        payloads = [own_payload] + [cross_swap(payloads[k], k, 1) for k in others]

        (*weights, gain), token = fetch(
            (w_query, w_forget, w_input, w_outgate, norm_gain[None]), own_payload
        )
        own, *sent = call(
            functools.partial(project_kernel, n_ep),
            [((batch, 4 * channels), F32)] + [((batch, 4 * channels), BF16)] * (n_ep - 1),
            [VMEM] * (n_ep + 6),
            (*payloads, gain, *weights, token),
            flops=8 * rows * block * channels,
        )
        got = [ep_swap(sent[k - 1], k) for k in others]
        (state, full, router_t), token = fetch((recurrent_state, tokens, w_router.T), own)
        inverse, router = call(
            inverse_kernel,
            [((batch, LANES), F32), ((w_router.shape[1] + 8, width), BF16)],
            [VMEM] * 3,
            (full, router_t, branch_gate[None]),
        )


        mixed, gates = call(
            functools.partial(read_kernel, n_ep),
            [((batch, channels + LANES), BF16), ((batch, 3 * channels), F32)],
            [VMEM] * (n_ep + 6),
            (own, *got, inverse, forget_floor[None], head_gain[None], state, routes.T, token),
            [pltpu.VMEM((batch, channels), F32)],
            flops=1 << 24,
        )
        mixed_all = [mixed] + [ep_swap(mixed, k) for k in others]

        group = 4
        new_state, token = pl.pallas_call(
            functools.partial(update_kernel, group),
            out_shape=[
                jax.ShapeDtypeStruct(recurrent_state.shape, F32),
                jax.ShapeDtypeStruct((8, LANES), F32),
            ],
            in_specs=[VMEM] * 2,
            out_specs=[HBM, VMEM],
            scratch_shapes=[
                pltpu.VMEM(recurrent_state.shape, F32),
                pltpu.SemaphoreType.DMA((batch // group,)),
            ],
            cost_estimate=pl.CostEstimate(flops=1 << 26, bytes_accessed=0, transcendentals=0),
            compiler_params=pltpu.CompilerParams(vmem_limit_bytes=16 << 20),
        )(gates, state)

        give, keep = call(
            functools.partial(output_kernel, n_ep),
            [((rows, half), BF16), ((rows, half), F32)],
            [VMEM] * (n_ep + 2),
            (*mixed_all, w_output, token),
            flops=2 * rows * channels * block,
        )
        core = core_swap(give)
        (summed,) = call(add_kernel, [((rows, half), BF16)], [VMEM] * 2, (keep, core))
        along = [z_swap(summed, m, m & 1) for m in range(1, n_z)]
        (gate_w, up_w), token = fetch(
            (jnp.swapaxes(expert_gate, 1, 2), jnp.swapaxes(expert_up, 1, 2)), summed
        )
        (part,) = call(
            functools.partial(hidden_kernel, n_ep),
            [((rows, half), BF16)],
            [VMEM] * (n_ep + n_z + 2),
            (*payloads, keep, core, *along, token),
        )

        pieces = [part] + [cross_swap(part, k, k & 1) for k in others]
        sibling = core_swap(part)
        padded = -(-shared_width // LANES) * LANES
        shared_own, shared_sent = call(
            shared_kernel,
            [((rows, 2 * padded), F32), ((rows, 2 * padded), BF16)],
            [VMEM] * 5,
            (
                part, sibling, ffn_gain[None],
                jnp.swapaxes(shared_gate_w, 0, 1), jnp.swapaxes(shared_up_w, 0, 1),
            ),
            flops=4 * rows * block * shared_width,
        )
        siblings = [sibling] + [core_swap(pieces[k]) for k in others]
        shared_got = [ep_swap(shared_sent, k) for k in others]

        inner, scales, own_hidden, down_w = call(
            functools.partial(expert_kernel, n_ep),
            [
                ((rows, local * inner_width), BF16),
                ((rows, LANES), F32),
                ((batch, slice_width), F32),
                ((local * inner_width, width), BF16),
            ],
            [VMEM] * (3 * n_ep + 4) + [HBM],
            (
                *pieces, *siblings, *mixed_all, ffn_gain[None], router, gate_w, up_w,
                pltpu.with_memory_space_constraint(expert_down, pltpu.HBM),
            ),
            [
                pltpu.VMEM((rows, width), F32),
                pltpu.VMEM((rows, width), BF16),
                pltpu.SemaphoreType.DMA((local,)),
            ],
            flops=4 * rows * width * inner_width * local,
        )

        give, shared = call(
            functools.partial(down_kernel, n_ep, n_z, False),
            [((rows, side), BF16), ((rows, shared_width), BF16)],
            [VMEM] * (n_ep + 4),
            (inner, shared_own, *shared_got, scales, down_w, shared_down_w),
            flops=rows * width * inner_width * local,
        )
        core = core_swap(give)
        (keep,) = call(
            functools.partial(down_kernel, n_ep, n_z, True),
            [((rows, side), F32)],
            [VMEM] * 4,
            (inner, shared, down_w, shared_down_w),
            flops=rows * width * inner_width * local,
        )
        own, *sent = call(
            functools.partial(merge_kernel, n_ep),
            [((batch, side), F32)] + [((batch, side), BF16)] * (n_ep - 1),
            [VMEM] * 2,
            (keep, core),
        )
        got = [ep_swap(sent[k - 1], k) for k in others]
        base, *sent = call(
            functools.partial(gather_kernel, n_ep, n_z),
            [((batch, slice_width), F32)] + [((batch, slice_width), BF16)] * (n_z - 1),
            [VMEM] * (n_ep + 1),
            (own, *got, own_hidden),
            [pltpu.VMEM((batch, side), F32)],
        )
        got = [z_swap(sent[m - 1], m) for m in range(1, n_z)]
        (layer_out,) = call(
            finish_kernel, [((batch, slice_width), BF16)], [VMEM] * n_z, (base, *got)
        )
        return layer_out, new_state

    return body


def solution(mesh):
    body = make_body(mesh.shape["ep"], mesh.shape["tp"])

    return jax.shard_map(
        body,
        mesh=mesh,
        in_specs=(
            P("ep", None),
            P(),
            P("ep", "tp"),
            P("ep", "tp"),
            P("ep", "tp"),
            P("ep", "tp"),
            P("tp"),
            P("tp"),
            P("ep", "tp", None, None),
            P("tp", "ep"),
            P(),
            P(),
            P("ep", None),
            P("ep", None, "tp"),
            P("ep", None, "tp"),
            P("ep", "tp", None),
            P("ep", "tp"),
            P("ep", "tp"),
            P("tp", "ep"),
            P(),
        ),
        out_specs=(P("ep", "tp"), P("ep", "tp", None, None)),
        check_vma=False,
    )
```

```python
import functools

import jax
import jax.numpy as jnp
from jax import lax
from jax.experimental import pallas as pl
from jax.experimental.pallas import tpu as pltpu
from jax.sharding import PartitionSpec as P


NORM_EPSILON = 1e-06
ROUTED_SCALE = 2.5
LANES = 128
F32 = jnp.float32
BF16 = jnp.bfloat16
VMEM = pl.BlockSpec(memory_space=pltpu.VMEM)
HBM = pl.BlockSpec(memory_space=pltpu.HBM)


def dot(a, b):
    return jnp.dot(a, b, preferred_element_type=F32)


def dot_t(a, b):
    return lax.dot_general(a, b, (((1,), (1,)), ((), ())), preferred_element_type=F32)


def silu(x):
    return x * jax.nn.sigmoid(x)


def swap(value, axis, size, step):
    return lax.ppermute(value, axis, [(s, s ^ step) for s in range(size)])


def inverse_rms(floats):
    return lax.rsqrt(jnp.mean(floats * floats, axis=-1, keepdims=True) + NORM_EPSILON)


def lane_slice(index, size):
    return pl.ds(pl.multiple_of(index * size, LANES), size)


def half_index():
    t = lax.axis_index("tp")
    return lax.rem(t + lax.div(t, 4) + lax.div(lax.axis_index("ep"), 2), 2)


def call(body, outs, ins, args, scratch=(), flops=0, limit=24):
    return pl.pallas_call(
        body,
        out_shape=[jax.ShapeDtypeStruct(s, d) for s, d in outs],
        in_specs=ins,
        out_specs=[VMEM] * len(outs),
        scratch_shapes=list(scratch),
        cost_estimate=pl.CostEstimate(flops=flops, bytes_accessed=0, transcendentals=0),
        compiler_params=pltpu.CompilerParams(vmem_limit_bytes=limit << 20),
    )(*args)


def prepare_kernel(tokens, *refs):
    outs, sems = refs[:-1], refs[-1]
    e = lax.axis_index("ep")
    block = outs[0].shape[1]
    copies = [
        pltpu.make_async_copy(tokens.at[:, lane_slice(e ^ k, block)], out, sems.at[k])
        for k, out in enumerate(outs)
    ]
    for copy in copies:
        copy.start()
    for copy in copies:
        copy.wait()


def route_mask(routes_t):
    batch = routes_t.shape[1]
    names = lax.broadcasted_iota(jnp.int32, (LANES, batch), 0)
    hit = names == routes_t[0:1, :]
    for j in range(1, routes_t.shape[0]):
        hit = hit | (names == routes_t[j : j + 1, :])
    eye = lax.broadcasted_iota(jnp.int32, (batch, batch), 0) == lax.broadcasted_iota(
        jnp.int32, (batch, batch), 1
    )
    return dot_t(jnp.where(eye, 1.0, 0.0).astype(BF16), jnp.where(hit, 1.0, 0.0).astype(BF16))


def fetch_kernel(arrays, *refs):
    sources, copied, token, sems = refs[:arrays], refs[-arrays - 2 : -2], refs[-2], refs[-1]
    copies = []
    for source, target in zip(sources, copied, strict=True):
        rows = target.shape[0]
        whole = 1 if target.ndim == 2 else rows
        parts = 4 if rows % (32 if target.ndim == 2 else 4) == 0 else whole
        step = rows // parts
        for p in range(parts):
            span = pl.ds(p * step, step)
            copies.append(
                pltpu.make_async_copy(source.at[span], target.at[span], sems.at[len(copies)])
            )
    for copy in copies:
        copy.start()
    for copy in copies:
        copy.wait()
    token[...] = jnp.zeros_like(token)


def fetch(arrays, after):
    arrays = [pltpu.with_memory_space_constraint(a, pltpu.HBM) for a in arrays]
    *copied, token = call(
        functools.partial(fetch_kernel, len(arrays)),
        [(a.shape, a.dtype) for a in arrays] + [((8, LANES), F32)],
        [HBM] * len(arrays) + [VMEM] * len(after),
        (*arrays, *after),
        [pltpu.SemaphoreType.DMA((24 * len(arrays),))],
        flops=1 << 26,
        limit=1,
    )
    return copied, token


def inverse_kernel(tokens, router_t, branch, routes_t, out, router, mask):
    mask[...] = route_mask(routes_t[...]).astype(BF16)
    out[...] = jnp.broadcast_to(inverse_rms(tokens[...].astype(F32)), out.shape)
    extra = jnp.broadcast_to(branch[...].astype(F32), (8, branch.shape[1]))
    router[...] = jnp.concatenate([router_t[...].astype(F32), extra], axis=0).astype(BF16)


def project_kernel(n_ep, *refs):
    payloads, gain, weights = refs[:n_ep], refs[n_ep], refs[n_ep + 1 : n_ep + 5]
    own, sent = refs[n_ep + 6], refs[n_ep + 7 :]
    batch = own.shape[0]
    block, channels = weights[0].shape
    row = gain[:, lane_slice(lax.axis_index("ep"), block)]
    scaled = jnp.concatenate([p[...].astype(F32) for p in payloads], axis=0) * row
    scaled = scaled.astype(BF16)
    for i, weight in enumerate(weights):
        part = dot(scaled, weight[...])
        lanes = slice(i * channels, (i + 1) * channels)
        own[:, lanes] = part[:batch]
        for k in range(1, n_ep):
            sent[k - 1][:, lanes] = part[k * batch : (k + 1) * batch].astype(BF16)


def columns_of(value):
    rows, lanes = value.shape
    return jnp.concatenate([value, jnp.zeros((LANES - rows, lanes), F32)], axis=0).T


def read_kernel(n_ep, *refs):
    own, got = refs[0], refs[1:n_ep]
    inverse, floor, head_gain, state, mask = refs[n_ep : n_ep + 5]
    mixed, gates, scratch = refs[n_ep + 6 :]
    batch, heads, size = state.shape[:3]
    channels = heads * size
    total = own[...]
    for g in got:
        total = total + g[...].astype(F32)
    total = total * inverse[:, 0:1]
    query, forget_pre, value, out_gate = (
        total[:, i * channels : (i + 1) * channels] for i in range(4)
    )
    low = floor[...]
    forget = low + (1.0 - low) * jax.nn.sigmoid(forget_pre)
    key = (1.0 - low) * jax.nn.sigmoid(-forget_pre)
    gates[:, :channels] = forget
    gates[:, channels : 2 * channels] = key
    gates[:, 2 * channels :] = value
    active = silu(query)
    weight = columns_of(active * forget)
    for b in range(batch):
        for h in range(heads):
            column = weight[h * size : (h + 1) * size, b : b + 1]
            scratch[b : b + 1, h * size : (h + 1) * size] = jnp.sum(
                column * state[b, h], axis=0, keepdims=True
            )
    mixed[:, channels:] = mask[...]
    scale = head_gain[...] * silu(out_gate)
    for h in range(heads):
        lanes = slice(h * size, (h + 1) * size)
        read = scratch[:, lanes] + value[:, lanes] * jnp.sum(
            active[:, lanes] * key[:, lanes], axis=-1, keepdims=True
        )
        mixed[:, lanes] = (read * inverse_rms(read) * scale[:, lanes]).astype(BF16)


def update_kernel(group, gates, state, out, token, buffer, sems):
    batch, heads, size = state.shape[:3]
    channels = heads * size
    forget = columns_of(gates[:, :channels])
    key = columns_of(gates[:, channels : 2 * channels])
    copies = []
    for b in range(batch):
        for h in range(heads):
            rows = slice(h * size, (h + 1) * size)
            value = gates[b : b + 1, 2 * channels + h * size : 2 * channels + (h + 1) * size]
            buffer[b, h] = forget[rows, b : b + 1] * state[b, h] + key[rows, b : b + 1] * value
        if (b + 1) % group == 0:
            span = pl.ds(b + 1 - group, group)
            copies.append(
                pltpu.make_async_copy(buffer.at[span], out.at[span], sems.at[len(copies)])
            )
            copies[-1].start()
    for copy in copies:
        copy.wait()
    token[...] = jnp.zeros_like(token)


def output_kernel(n_ep, *refs):
    mixed, weight, give, keep = refs[:n_ep], refs[n_ep], refs[-2], refs[-1]
    c = half_index()
    half = keep.shape[1]
    rows = jnp.concatenate([m[...].astype(F32) for m in mixed], axis=0).astype(BF16)
    rows = rows[:, : weight.shape[0]]
    give[...] = dot(rows, weight[:, lane_slice(1 - c, half)]).astype(BF16)
    keep[...] = dot(rows, weight[:, lane_slice(c, half)])


def add_kernel(keep, got, out):
    out[...] = (keep[...] + got[...].astype(F32)).astype(BF16)


def hidden_kernel(n_ep, *refs):
    payloads, keep, core, others = refs[:n_ep], refs[n_ep], refs[n_ep + 1], refs[n_ep + 2 : -2]
    out = refs[-1]
    c = half_index()
    half = keep.shape[1]
    total = jnp.concatenate([p[:, lane_slice(c, half)].astype(F32) for p in payloads], axis=0)
    mixed = keep[...] + core[...].astype(F32)
    for other in others:
        mixed = mixed + other[...].astype(F32)
    out[...] = (total + mixed).astype(BF16)


def shared_kernel(mine, other, gain, gate_t, up_t, own, sent):
    c = half_index()
    e = lax.axis_index("ep")
    half = mine.shape[1]
    inner, padded = gate_t.shape[0], own.shape[1] // 2
    own[...] = jnp.zeros_like(own)
    total = [None, None]
    for piece, h in ((mine, c), (other, 1 - c)):
        row = gain[:, lane_slice(2 * e + h, half)]
        scaled = (piece[...].astype(F32) * row).astype(BF16)
        for i, weight in enumerate((gate_t, up_t)):
            part = dot_t(scaled, weight[:, lane_slice(h, half)])
            total[i] = part if total[i] is None else total[i] + part
    for i in range(2):
        own[:, i * padded : i * padded + inner] = total[i]
    sent[...] = own[...].astype(BF16)


def expert_kernel(n_ep, *refs):
    pieces, others, payloads = refs[:n_ep], refs[n_ep : 2 * n_ep], refs[2 * n_ep : 3 * n_ep]
    gain, router, gate_w, up_w, down = refs[3 * n_ep : 3 * n_ep + 5]
    inner, scales, own_hidden, down_out, x_ref, n_ref, sems = refs[3 * n_ep + 5 :]
    local, inner_width = gate_w.shape[:2]
    spans = [slice(i * inner_width, (i + 1) * inner_width) for i in range(local)]
    fetches = [
        pltpu.make_async_copy(down.at[i], down_out.at[spans[i]], sems.at[i])
        for i in range(local)
    ]
    for copy in fetches:
        copy.start()
    e = lax.axis_index("ep")
    t = lax.axis_index("tp")
    c = half_index()
    rows, half = pieces[0].shape
    batch = rows // n_ep
    squares = jnp.zeros((rows, half), F32)
    for k in range(n_ep):
        for source, h in ((pieces[k], c), (others[k], 1 - c)):
            floats = source[...].astype(F32)
            floats = jnp.concatenate(
                [floats[(j ^ k) * batch : ((j ^ k) + 1) * batch] for j in range(n_ep)], axis=0
            )
            squares = squares + floats * floats
            x_ref[:, lane_slice(2 * (e ^ k) + h, half)] = floats
    width = x_ref.shape[1]
    inv = lax.rsqrt(jnp.sum(squares, axis=-1, keepdims=True) / width + NORM_EPSILON)
    own_hidden[...] = x_ref[:batch, lane_slice(t, own_hidden.shape[1])]
    n_ref[...] = (x_ref[...] * inv * gain[...]).astype(BF16)
    scores = jax.nn.sigmoid(dot_t(n_ref[...], router[...]))
    experts = router.shape[0] - 8
    lane = lax.broadcasted_iota(jnp.int32, scores.shape, 1)
    start = payloads[0].shape[1] - LANES
    mask = jnp.concatenate([p[:, start:].astype(F32) for p in payloads], axis=0)
    chosen = jnp.where(mask[:, : router.shape[0]] > 0.5, scores, 0.0)
    weights = chosen / jnp.sum(chosen, axis=1, keepdims=True) * ROUTED_SCALE
    branch = jnp.sum(jnp.where(lane == experts, scores, 0.0), axis=1, keepdims=True)
    spread = lax.broadcasted_iota(jnp.int32, scales.shape, 1)
    scales[...] = jnp.where(spread == 0, inv, branch)
    for i in range(local):
        combine = jnp.sum(jnp.where(lane == e * local + i, weights, 0.0), axis=1, keepdims=True)
        gate = dot_t(n_ref[...], gate_w[i])
        up = dot_t(n_ref[...], up_w[i])
        inner[:, spans[i]] = (silu(gate) * up * combine).astype(BF16)
    for copy in fetches:
        copy.wait()


def shared_activation(n_ep, shape, own, *refs):
    got, scales = refs[:-1], refs[-1]
    rows, width = shape
    batch = rows // n_ep
    total = own[...]
    for k in range(1, n_ep):
        floats = got[k - 1][...].astype(F32)
        total = total + jnp.concatenate(
            [floats[(j ^ k) * batch : ((j ^ k) + 1) * batch] for j in range(n_ep)], axis=0
        )
    total = total * scales[:, 0:1]
    padded = total.shape[1] // 2
    shared = silu(total[:, :padded]) * total[:, padded:] * scales[:, 1:2]
    return shared[:, :width].astype(BF16)


def down_kernel(n_ep, n_z, mine, inner, *refs):
    if mine:
        shared, weight, shared_down, out = refs
    else:
        *refs, weight, shared_down, out, shared = refs
        shared[...] = shared_activation(n_ep, shared.shape, *refs)
    e = lax.axis_index("ep")
    c = lax.rem(lax.axis_index("tp"), 2)
    h = c if mine else 1 - c
    size = weight.shape[1] // (2 * n_z)
    ratio = shared_down.shape[1] // size
    for z in range(n_z):
        lanes = lane_slice(2 * z + h, size)
        part = dot(inner[...], weight[:, lanes])
        out[:, z * size : (z + 1) * size] = part.astype(out.dtype)
    for z in range(n_z):
        q = 2 * z + h

        @pl.when(lax.div(q, ratio) == e)
        def _():
            lanes = slice(z * size, (z + 1) * size)
            extra = dot(shared[...], shared_down[:, lane_slice(lax.rem(q, ratio), size)])
            out[:, lanes] = (out[:, lanes].astype(F32) + extra).astype(out.dtype)


def merge_kernel(n_ep, keep, got, own, *sent):
    batch = own.shape[0]
    total = keep[...] + got[...].astype(F32)
    own[...] = total[:batch]
    for k in range(1, n_ep):
        sent[k - 1][...] = total[k * batch : (k + 1) * batch].astype(BF16)


def gather_kernel(n_ep, n_z, *refs):
    own, got = refs[0], refs[1:n_ep]
    hidden, base, sent, scratch = refs[n_ep], refs[n_ep + 1], refs[n_ep + 2 : -1], refs[-1]
    z = lax.div(lax.axis_index("tp"), 2)
    size = base.shape[1]
    total = own[...]
    for g in got:
        total = total + g[...].astype(F32)
    scratch[...] = total
    base[...] = hidden[...] + scratch[:, lane_slice(z, size)]
    for m in range(1, n_z):
        sent[m - 1][...] = scratch[:, lane_slice(z ^ m, size)].astype(BF16)


def finish_kernel(*refs):
    total = refs[0][...]
    for r in refs[1:-1]:
        total = total + r[...].astype(F32)
    refs[-1][...] = total.astype(BF16)


def make_body(n_ep, n_tp):
    n_z = n_tp // 2

    def ep_swap(value, k):
        return swap(value, "ep", n_ep, k)

    def cross_swap(value, k, flip):
        pairs = [
            (e * n_tp + t, (e ^ k) * n_tp + (t ^ flip)) for e in range(n_ep) for t in range(n_tp)
        ]
        return lax.ppermute(value, ("ep", "tp"), pairs)

    def z_swap(value, m, flip=0):
        return swap(value, "tp", n_tp, 2 * m | flip)

    def core_swap(value):
        return swap(value, "tp", n_tp, 1)

    def body(
        tokens, norm_gain, w_query, w_forget, w_input, w_outgate, forget_floor, head_gain,
        recurrent_state, w_output, ffn_gain, w_router, routes, expert_gate, expert_up,
        expert_down, shared_gate_w, shared_up_w, shared_down_w, branch_gate,
    ):
        batch, width = tokens.shape
        rows = n_ep * batch
        block = width // n_ep
        half = block // 2
        heads, size = recurrent_state.shape[1:3]
        channels = heads * size
        local, _, inner_width = expert_gate.shape
        shared_width = shared_gate_w.shape[1]
        slice_width = width // n_tp
        side = n_z * slice_width
        others = range(1, n_ep)

        payloads = call(
            prepare_kernel,
            [((batch, block), BF16)] * n_ep,
            [HBM],
            (pltpu.with_memory_space_constraint(tokens, pltpu.HBM),),
            [pltpu.SemaphoreType.DMA((n_ep,))],
        )
        own_payload = payloads[0]
        payloads = [own_payload] + [cross_swap(payloads[k], k, 1) for k in others]

        branch_row = branch_gate[None]
        (*weights, gain), token = fetch(
            (w_query, w_forget, w_input, w_outgate, norm_gain[None]), (own_payload, branch_row)
        )
        own, *sent = call(
            functools.partial(project_kernel, n_ep),
            [((batch, 4 * channels), F32)] + [((batch, 4 * channels), BF16)] * (n_ep - 1),
            [VMEM] * (n_ep + 6),
            (*payloads, gain, *weights, token),
            flops=8 * rows * block * channels,
        )
        got = [ep_swap(sent[k - 1], k) for k in others]
        (state, full, router_t), token = fetch((recurrent_state, tokens, w_router.T), (own,))
        inverse, router, mask = call(
            inverse_kernel,
            [
                ((batch, LANES), F32),
                ((w_router.shape[1] + 8, width), BF16),
                ((batch, LANES), BF16),
            ],
            [VMEM] * 4,
            (full, router_t, branch_row, routes.T),
        )


        mixed, gates = call(
            functools.partial(read_kernel, n_ep),
            [((batch, channels + LANES), BF16), ((batch, 3 * channels), F32)],
            [VMEM] * (n_ep + 6),
            (own, *got, inverse, forget_floor[None], head_gain[None], state, mask, token),
            [pltpu.VMEM((batch, channels), F32)],
            flops=1 << 24,
        )
        mixed_all = [mixed] + [ep_swap(mixed, k) for k in others]

        group = 4
        new_state, token = pl.pallas_call(
            functools.partial(update_kernel, group),
            out_shape=[
                jax.ShapeDtypeStruct(recurrent_state.shape, F32),
                jax.ShapeDtypeStruct((8, LANES), F32),
            ],
            in_specs=[VMEM] * 2,
            out_specs=[HBM, VMEM],
            scratch_shapes=[
                pltpu.VMEM(recurrent_state.shape, F32),
                pltpu.SemaphoreType.DMA((batch // group,)),
            ],
            cost_estimate=pl.CostEstimate(flops=1 << 26, bytes_accessed=0, transcendentals=0),
            compiler_params=pltpu.CompilerParams(vmem_limit_bytes=16 << 20),
        )(gates, state)

        give, keep = call(
            functools.partial(output_kernel, n_ep),
            [((rows, half), BF16), ((rows, half), F32)],
            [VMEM] * (n_ep + 2),
            (*mixed_all, w_output, token),
            flops=2 * rows * channels * block,
        )
        core = core_swap(give)
        (summed,) = call(add_kernel, [((rows, half), BF16)], [VMEM] * 2, (keep, core))
        along = [z_swap(summed, m, (m >> 1) & 1) for m in range(1, n_z)]
        (gate_w, up_w), token = fetch(
            (jnp.swapaxes(expert_gate, 1, 2), jnp.swapaxes(expert_up, 1, 2)), (summed,)
        )
        (part,) = call(
            functools.partial(hidden_kernel, n_ep),
            [((rows, half), BF16)],
            [VMEM] * (n_ep + n_z + 2),
            (*payloads, keep, core, *along, token),
        )

        pieces = [part] + [cross_swap(part, k, (k >> 1) & 1) for k in others]
        sibling = core_swap(part)
        padded = -(-shared_width // LANES) * LANES
        shared_own, shared_sent = call(
            shared_kernel,
            [((rows, 2 * padded), F32), ((rows, 2 * padded), BF16)],
            [VMEM] * 5,
            (
                part, sibling, ffn_gain[None],
                jnp.swapaxes(shared_gate_w, 0, 1), jnp.swapaxes(shared_up_w, 0, 1),
            ),
            flops=4 * rows * block * shared_width,
        )
        siblings = [sibling] + [core_swap(pieces[k]) for k in others]
        shared_got = [ep_swap(shared_sent, k) for k in others]

        inner, scales, own_hidden, down_w = call(
            functools.partial(expert_kernel, n_ep),
            [
                ((rows, local * inner_width), BF16),
                ((rows, LANES), F32),
                ((batch, slice_width), F32),
                ((local * inner_width, width), BF16),
            ],
            [VMEM] * (3 * n_ep + 4) + [HBM],
            (
                *pieces, *siblings, *mixed_all, ffn_gain[None], router, gate_w, up_w,
                pltpu.with_memory_space_constraint(expert_down, pltpu.HBM),
            ),
            [
                pltpu.VMEM((rows, width), F32),
                pltpu.VMEM((rows, width), BF16),
                pltpu.SemaphoreType.DMA((local,)),
            ],
            flops=4 * rows * width * inner_width * local,
        )

        give, shared = call(
            functools.partial(down_kernel, n_ep, n_z, False),
            [((rows, side), BF16), ((rows, shared_width), BF16)],
            [VMEM] * (n_ep + 4),
            (inner, shared_own, *shared_got, scales, down_w, shared_down_w),
            flops=rows * width * inner_width * local,
        )
        core = core_swap(give)
        (keep,) = call(
            functools.partial(down_kernel, n_ep, n_z, True),
            [((rows, side), F32)],
            [VMEM] * 4,
            (inner, shared, down_w, shared_down_w),
            flops=rows * width * inner_width * local,
        )
        own, *sent = call(
            functools.partial(merge_kernel, n_ep),
            [((batch, side), F32)] + [((batch, side), BF16)] * (n_ep - 1),
            [VMEM] * 2,
            (keep, core),
        )
        got = [ep_swap(sent[k - 1], k) for k in others]
        base, *sent = call(
            functools.partial(gather_kernel, n_ep, n_z),
            [((batch, slice_width), F32)] + [((batch, slice_width), BF16)] * (n_z - 1),
            [VMEM] * (n_ep + 1),
            (own, *got, own_hidden),
            [pltpu.VMEM((batch, side), F32)],
        )
        got = [z_swap(sent[m - 1], m) for m in range(1, n_z)]
        (layer_out,) = call(
            finish_kernel, [((batch, slice_width), BF16)], [VMEM] * n_z, (base, *got)
        )
        return layer_out, new_state

    return body


def solution(mesh):
    body = make_body(mesh.shape["ep"], mesh.shape["tp"])

    return jax.shard_map(
        body,
        mesh=mesh,
        in_specs=(
            P("ep", None),
            P(),
            P("ep", "tp"),
            P("ep", "tp"),
            P("ep", "tp"),
            P("ep", "tp"),
            P("tp"),
            P("tp"),
            P("ep", "tp", None, None),
            P("tp", "ep"),
            P(),
            P(),
            P("ep", None),
            P("ep", None, "tp"),
            P("ep", None, "tp"),
            P("ep", "tp", None),
            P("ep", "tp"),
            P("ep", "tp"),
            P("tp", "ep"),
            P(),
        ),
        out_specs=(P("ep", "tp"), P("ep", "tp", None, None)),
        check_vma=False,
    )
```

```python
import functools

import jax
import jax.numpy as jnp
from jax import lax
from jax.experimental import pallas as pl
from jax.experimental.pallas import tpu as pltpu
from jax.sharding import PartitionSpec as P


NORM_EPSILON = 1e-06
ROUTED_SCALE = 2.5
LANES = 128
F32 = jnp.float32
BF16 = jnp.bfloat16
VMEM = pl.BlockSpec(memory_space=pltpu.VMEM)
HBM = pl.BlockSpec(memory_space=pltpu.HBM)


def dot(a, b):
    return jnp.dot(a, b, preferred_element_type=F32)


def dot_t(a, b):
    return lax.dot_general(a, b, (((1,), (1,)), ((), ())), preferred_element_type=F32)


def silu(x):
    return x * jax.nn.sigmoid(x)


def swap(value, axis, size, step):
    return lax.ppermute(value, axis, [(s, s ^ step) for s in range(size)])


def inverse_rms(floats):
    return lax.rsqrt(jnp.mean(floats * floats, axis=-1, keepdims=True) + NORM_EPSILON)


def lane_slice(index, size):
    return pl.ds(pl.multiple_of(index * size, LANES), size)


def half_index():
    t = lax.axis_index("tp")
    return lax.rem(t + lax.div(t, 4) + lax.div(lax.axis_index("ep"), 2), 2)


def call(body, outs, ins, args, scratch=(), flops=0, limit=24):
    return pl.pallas_call(
        body,
        out_shape=[jax.ShapeDtypeStruct(s, d) for s, d in outs],
        in_specs=ins,
        out_specs=[VMEM] * len(outs),
        scratch_shapes=list(scratch),
        cost_estimate=pl.CostEstimate(flops=flops, bytes_accessed=0, transcendentals=0),
        compiler_params=pltpu.CompilerParams(vmem_limit_bytes=limit << 20),
    )(*args)


def prepare_kernel(tokens, *refs):
    outs, sems = refs[:-1], refs[-1]
    e = lax.axis_index("ep")
    block = outs[0].shape[1]
    copies = [
        pltpu.make_async_copy(tokens.at[:, lane_slice(e ^ k, block)], out, sems.at[k])
        for k, out in enumerate(outs)
    ]
    for copy in copies:
        copy.start()
    for copy in copies:
        copy.wait()


def route_mask(routes_t):
    batch = routes_t.shape[1]
    names = lax.broadcasted_iota(jnp.int32, (LANES, batch), 0)
    hit = names == routes_t[0:1, :]
    for j in range(1, routes_t.shape[0]):
        hit = hit | (names == routes_t[j : j + 1, :])
    eye = lax.broadcasted_iota(jnp.int32, (batch, batch), 0) == lax.broadcasted_iota(
        jnp.int32, (batch, batch), 1
    )
    return dot_t(jnp.where(eye, 1.0, 0.0).astype(BF16), jnp.where(hit, 1.0, 0.0).astype(BF16))


def fetch_kernel(arrays, *refs):
    sources, copied, token, sems = refs[:arrays], refs[-arrays - 2 : -2], refs[-2], refs[-1]
    copies = []
    for source, target in zip(sources, copied, strict=True):
        rows = target.shape[0]
        whole = 1 if target.ndim == 2 else rows
        parts = 4 if rows % (32 if target.ndim == 2 else 4) == 0 else whole
        step = rows // parts
        for p in range(parts):
            span = pl.ds(p * step, step)
            copies.append(
                pltpu.make_async_copy(source.at[span], target.at[span], sems.at[len(copies)])
            )
    for copy in copies:
        copy.start()
    for copy in copies:
        copy.wait()
    token[...] = jnp.zeros_like(token)


def fetch(arrays, after):
    arrays = [pltpu.with_memory_space_constraint(a, pltpu.HBM) for a in arrays]
    *copied, token = call(
        functools.partial(fetch_kernel, len(arrays)),
        [(a.shape, a.dtype) for a in arrays] + [((8, LANES), F32)],
        [HBM] * len(arrays) + [VMEM] * len(after),
        (*arrays, *after),
        [pltpu.SemaphoreType.DMA((24 * len(arrays),))],
        flops=1 << 26,
        limit=1,
    )
    return copied, token


def inverse_kernel(tokens, router_t, branch, routes_t, out, router, mask):
    mask[...] = route_mask(routes_t[...]).astype(BF16)
    out[...] = jnp.broadcast_to(inverse_rms(tokens[...].astype(F32)), out.shape)
    extra = jnp.broadcast_to(branch[...].astype(F32), (8, branch.shape[1]))
    router[...] = jnp.concatenate([router_t[...].astype(F32), extra], axis=0).astype(BF16)


def project_kernel(n_ep, *refs):
    payloads, gain, weights = refs[:n_ep], refs[n_ep], refs[n_ep + 1 : n_ep + 5]
    own, sent = refs[n_ep + 6], refs[n_ep + 7 :]
    batch = own.shape[0]
    block, channels = weights[0].shape
    row = gain[:, lane_slice(lax.axis_index("ep"), block)]
    scaled = jnp.concatenate([p[...].astype(F32) for p in payloads], axis=0) * row
    scaled = scaled.astype(BF16)
    for i, weight in enumerate(weights):
        part = dot(scaled, weight[...])
        lanes = slice(i * channels, (i + 1) * channels)
        own[:, lanes] = part[:batch]
        for k in range(1, n_ep):
            sent[k - 1][:, lanes] = part[k * batch : (k + 1) * batch].astype(BF16)


def columns_of(value):
    rows, lanes = value.shape
    return jnp.concatenate([value, jnp.zeros((LANES - rows, lanes), F32)], axis=0).T


def read_kernel(n_ep, *refs):
    own, got = refs[0], refs[1:n_ep]
    inverse, floor, head_gain, state, mask = refs[n_ep : n_ep + 5]
    mixed, gates, scratch = refs[n_ep + 6 :]
    batch, heads, size = state.shape[:3]
    channels = heads * size
    total = own[...]
    for g in got:
        total = total + g[...].astype(F32)
    total = total * inverse[:, 0:1]
    query, forget_pre, value, out_gate = (
        total[:, i * channels : (i + 1) * channels] for i in range(4)
    )
    low = floor[...]
    forget = low + (1.0 - low) * jax.nn.sigmoid(forget_pre)
    key = (1.0 - low) * jax.nn.sigmoid(-forget_pre)
    gates[:, :channels] = forget
    gates[:, channels : 2 * channels] = key
    gates[:, 2 * channels :] = value
    active = silu(query)
    weight = columns_of(active * forget)
    for b in range(batch):
        for h in range(heads):
            column = weight[h * size : (h + 1) * size, b : b + 1]
            scratch[b : b + 1, h * size : (h + 1) * size] = jnp.sum(
                column * state[b, h], axis=0, keepdims=True
            )
    mixed[:, channels:] = mask[...]
    scale = head_gain[...] * silu(out_gate)
    for h in range(heads):
        lanes = slice(h * size, (h + 1) * size)
        read = scratch[:, lanes] + value[:, lanes] * jnp.sum(
            active[:, lanes] * key[:, lanes], axis=-1, keepdims=True
        )
        mixed[:, lanes] = (read * inverse_rms(read) * scale[:, lanes]).astype(BF16)


def update_kernel(group, gates, state, _, out, token, buffer, sems):
    batch, heads, size = state.shape[:3]
    channels = heads * size
    forget = columns_of(gates[:, :channels])
    key = columns_of(gates[:, channels : 2 * channels])
    copies = []
    for b in range(batch):
        for h in range(heads):
            rows = slice(h * size, (h + 1) * size)
            value = gates[b : b + 1, 2 * channels + h * size : 2 * channels + (h + 1) * size]
            buffer[b, h] = forget[rows, b : b + 1] * state[b, h] + key[rows, b : b + 1] * value
        if (b + 1) % group == 0:
            span = pl.ds(b + 1 - group, group)
            copies.append(
                pltpu.make_async_copy(buffer.at[span], out.at[span], sems.at[len(copies)])
            )
            copies[-1].start()
    for copy in copies:
        copy.wait()
    token[...] = jnp.zeros_like(token)


def output_kernel(n_ep, *refs):
    mixed, weight, give, keep = refs[:n_ep], refs[n_ep], refs[-2], refs[-1]
    c = half_index()
    half = keep.shape[1]
    rows = jnp.concatenate([m[...].astype(F32) for m in mixed], axis=0).astype(BF16)
    rows = rows[:, : weight.shape[0]]
    give[...] = dot(rows, weight[:, lane_slice(1 - c, half)]).astype(BF16)
    keep[...] = dot(rows, weight[:, lane_slice(c, half)])


def add_kernel(keep, got, out):
    out[...] = (keep[...] + got[...].astype(F32)).astype(BF16)


def hidden_kernel(n_ep, *refs):
    payloads, keep, core, others = refs[:n_ep], refs[n_ep], refs[n_ep + 1], refs[n_ep + 2 : -2]
    out = refs[-1]
    c = half_index()
    half = keep.shape[1]
    total = jnp.concatenate([p[:, lane_slice(c, half)].astype(F32) for p in payloads], axis=0)
    mixed = keep[...] + core[...].astype(F32)
    for other in others:
        mixed = mixed + other[...].astype(F32)
    out[...] = (total + mixed).astype(BF16)


def shared_kernel(mine, other, gain, gate_t, up_t, own, sent):
    c = half_index()
    e = lax.axis_index("ep")
    half = mine.shape[1]
    inner, padded = gate_t.shape[0], own.shape[1] // 2
    own[...] = jnp.zeros_like(own)
    total = [None, None]
    for piece, h in ((mine, c), (other, 1 - c)):
        row = gain[:, lane_slice(2 * e + h, half)]
        scaled = (piece[...].astype(F32) * row).astype(BF16)
        for i, weight in enumerate((gate_t, up_t)):
            part = dot_t(scaled, weight[:, lane_slice(h, half)])
            total[i] = part if total[i] is None else total[i] + part
    for i in range(2):
        own[:, i * padded : i * padded + inner] = total[i]
    sent[...] = own[...].astype(BF16)


def expert_kernel(n_ep, *refs):
    pieces, others, payloads = refs[:n_ep], refs[n_ep : 2 * n_ep], refs[2 * n_ep : 3 * n_ep]
    gain, router, gate_w, up_w, down = refs[3 * n_ep : 3 * n_ep + 5]
    inner, scales, own_hidden, down_out, x_ref, n_ref, sems = refs[3 * n_ep + 5 :]
    local, inner_width = gate_w.shape[:2]
    spans = [slice(i * inner_width, (i + 1) * inner_width) for i in range(local)]
    fetches = [
        pltpu.make_async_copy(down.at[i], down_out.at[spans[i]], sems.at[i])
        for i in range(local)
    ]
    for copy in fetches:
        copy.start()
    e = lax.axis_index("ep")
    t = lax.axis_index("tp")
    c = half_index()
    rows, half = pieces[0].shape
    batch = rows // n_ep
    squares = jnp.zeros((rows, half), F32)
    for k in range(n_ep):
        for source, h in ((pieces[k], c), (others[k], 1 - c)):
            floats = source[...].astype(F32)
            floats = jnp.concatenate(
                [floats[(j ^ k) * batch : ((j ^ k) + 1) * batch] for j in range(n_ep)], axis=0
            )
            squares = squares + floats * floats
            x_ref[:, lane_slice(2 * (e ^ k) + h, half)] = floats
    width = x_ref.shape[1]
    inv = lax.rsqrt(jnp.sum(squares, axis=-1, keepdims=True) / width + NORM_EPSILON)
    own_hidden[...] = x_ref[:batch, lane_slice(t, own_hidden.shape[1])]
    n_ref[...] = (x_ref[...] * inv * gain[...]).astype(BF16)
    scores = jax.nn.sigmoid(dot_t(n_ref[...], router[...]))
    experts = router.shape[0] - 8
    lane = lax.broadcasted_iota(jnp.int32, scores.shape, 1)
    start = payloads[0].shape[1] - LANES
    mask = jnp.concatenate([p[:, start:].astype(F32) for p in payloads], axis=0)
    chosen = jnp.where(mask[:, : router.shape[0]] > 0.5, scores, 0.0)
    weights = chosen / jnp.sum(chosen, axis=1, keepdims=True) * ROUTED_SCALE
    branch = jnp.sum(jnp.where(lane == experts, scores, 0.0), axis=1, keepdims=True)
    spread = lax.broadcasted_iota(jnp.int32, scales.shape, 1)
    scales[...] = jnp.where(spread == 0, inv, branch)
    for i in range(local):
        combine = jnp.sum(jnp.where(lane == e * local + i, weights, 0.0), axis=1, keepdims=True)
        gate = dot_t(n_ref[...], gate_w[i])
        up = dot_t(n_ref[...], up_w[i])
        inner[:, spans[i]] = (silu(gate) * up * combine).astype(BF16)
    for copy in fetches:
        copy.wait()


def shared_activation(n_ep, shape, own, *refs):
    got, scales = refs[:-1], refs[-1]
    rows, width = shape
    batch = rows // n_ep
    total = own[...]
    for k in range(1, n_ep):
        floats = got[k - 1][...].astype(F32)
        total = total + jnp.concatenate(
            [floats[(j ^ k) * batch : ((j ^ k) + 1) * batch] for j in range(n_ep)], axis=0
        )
    total = total * scales[:, 0:1]
    padded = total.shape[1] // 2
    shared = silu(total[:, :padded]) * total[:, padded:] * scales[:, 1:2]
    return shared[:, :width].astype(BF16)


def down_kernel(n_ep, n_z, mine, inner, *refs):
    if mine:
        shared, weight, shared_down, out = refs
    else:
        *refs, weight, shared_down, out, shared = refs
        shared[...] = shared_activation(n_ep, shared.shape, *refs)
    e = lax.axis_index("ep")
    c = lax.rem(lax.axis_index("tp"), 2)
    h = c if mine else 1 - c
    size = weight.shape[1] // (2 * n_z)
    ratio = shared_down.shape[1] // size
    for z in range(n_z):
        lanes = lane_slice(2 * z + h, size)
        part = dot(inner[...], weight[:, lanes])
        out[:, z * size : (z + 1) * size] = part.astype(out.dtype)
    for z in range(n_z):
        q = 2 * z + h

        @pl.when(lax.div(q, ratio) == e)
        def _():
            lanes = slice(z * size, (z + 1) * size)
            extra = dot(shared[...], shared_down[:, lane_slice(lax.rem(q, ratio), size)])
            out[:, lanes] = (out[:, lanes].astype(F32) + extra).astype(out.dtype)


def merge_kernel(n_ep, keep, got, own, *sent):
    batch = own.shape[0]
    total = keep[...] + got[...].astype(F32)
    own[...] = total[:batch]
    for k in range(1, n_ep):
        sent[k - 1][...] = total[k * batch : (k + 1) * batch].astype(BF16)


def gather_kernel(n_ep, n_z, *refs):
    own, got = refs[0], refs[1:n_ep]
    hidden, base, sent, scratch = refs[n_ep], refs[n_ep + 2], refs[n_ep + 3 : -1], refs[-1]
    z = lax.div(lax.axis_index("tp"), 2)
    size = base.shape[1]
    total = own[...]
    for g in got:
        total = total + g[...].astype(F32)
    scratch[...] = total
    base[...] = hidden[...] + scratch[:, lane_slice(z, size)]
    for m in range(1, n_z):
        sent[m - 1][...] = scratch[:, lane_slice(z ^ m, size)].astype(BF16)


def finish_kernel(*refs):
    total = refs[0][...]
    for r in refs[1:-1]:
        total = total + r[...].astype(F32)
    refs[-1][...] = total.astype(BF16)


def make_body(n_ep, n_tp):
    n_z = n_tp // 2

    def ep_swap(value, k):
        return swap(value, "ep", n_ep, k)

    def cross_swap(value, k, flip):
        pairs = [
            (e * n_tp + t, (e ^ k) * n_tp + (t ^ flip)) for e in range(n_ep) for t in range(n_tp)
        ]
        return lax.ppermute(value, ("ep", "tp"), pairs)

    def z_swap(value, m, flip=0):
        return swap(value, "tp", n_tp, 2 * m | flip)

    def core_swap(value):
        return swap(value, "tp", n_tp, 1)

    def body(
        tokens, norm_gain, w_query, w_forget, w_input, w_outgate, forget_floor, head_gain,
        recurrent_state, w_output, ffn_gain, w_router, routes, expert_gate, expert_up,
        expert_down, shared_gate_w, shared_up_w, shared_down_w, branch_gate,
    ):
        batch, width = tokens.shape
        rows = n_ep * batch
        block = width // n_ep
        half = block // 2
        heads, size = recurrent_state.shape[1:3]
        channels = heads * size
        local, _, inner_width = expert_gate.shape
        shared_width = shared_gate_w.shape[1]
        slice_width = width // n_tp
        side = n_z * slice_width
        others = range(1, n_ep)

        payloads = call(
            prepare_kernel,
            [((batch, block), BF16)] * n_ep,
            [HBM],
            (pltpu.with_memory_space_constraint(tokens, pltpu.HBM),),
            [pltpu.SemaphoreType.DMA((n_ep,))],
        )
        own_payload = payloads[0]
        payloads = [own_payload] + [cross_swap(payloads[k], k, 1) for k in others]

        branch_row = branch_gate[None]
        (*weights, gain), token = fetch(
            (w_query, w_forget, w_input, w_outgate, norm_gain[None]), (own_payload, branch_row)
        )
        own, *sent = call(
            functools.partial(project_kernel, n_ep),
            [((batch, 4 * channels), F32)] + [((batch, 4 * channels), BF16)] * (n_ep - 1),
            [VMEM] * (n_ep + 6),
            (*payloads, gain, *weights, token),
            flops=8 * rows * block * channels,
        )
        got = [ep_swap(sent[k - 1], k) for k in others]
        (state, full, router_t), token = fetch((recurrent_state, tokens, w_router.T), (own,))
        inverse, router, mask = call(
            inverse_kernel,
            [
                ((batch, LANES), F32),
                ((w_router.shape[1] + 8, width), BF16),
                ((batch, LANES), BF16),
            ],
            [VMEM] * 4,
            (full, router_t, branch_row, routes.T),
        )


        mixed, gates = call(
            functools.partial(read_kernel, n_ep),
            [((batch, channels + LANES), BF16), ((batch, 3 * channels), F32)],
            [VMEM] * (n_ep + 6),
            (own, *got, inverse, forget_floor[None], head_gain[None], state, mask, token),
            [pltpu.VMEM((batch, channels), F32)],
            flops=1 << 24,
        )
        mixed_all = [mixed] + [ep_swap(mixed, k) for k in others]

        give, keep = call(
            functools.partial(output_kernel, n_ep),
            [((rows, half), BF16), ((rows, half), F32)],
            [VMEM] * (n_ep + 1),
            (*mixed_all, w_output),
            flops=2 * rows * channels * block,
        )
        core = core_swap(give)
        (summed,) = call(add_kernel, [((rows, half), BF16)], [VMEM] * 2, (keep, core))
        along = [z_swap(summed, m, (m >> 1) & 1) for m in range(1, n_z)]
        (gate_w, up_w), token = fetch(
            (jnp.swapaxes(expert_gate, 1, 2), jnp.swapaxes(expert_up, 1, 2)), (summed,)
        )
        (part,) = call(
            functools.partial(hidden_kernel, n_ep),
            [((rows, half), BF16)],
            [VMEM] * (n_ep + n_z + 2),
            (*payloads, keep, core, *along, token),
        )

        pieces = [part] + [cross_swap(part, k, (k >> 1) & 1) for k in others]
        sibling = core_swap(part)
        padded = -(-shared_width // LANES) * LANES
        shared_own, shared_sent = call(
            shared_kernel,
            [((rows, 2 * padded), F32), ((rows, 2 * padded), BF16)],
            [VMEM] * 5,
            (
                part, sibling, ffn_gain[None],
                jnp.swapaxes(shared_gate_w, 0, 1), jnp.swapaxes(shared_up_w, 0, 1),
            ),
            flops=4 * rows * block * shared_width,
        )
        siblings = [sibling] + [core_swap(pieces[k]) for k in others]
        shared_got = [ep_swap(shared_sent, k) for k in others]

        inner, scales, own_hidden, down_w = call(
            functools.partial(expert_kernel, n_ep),
            [
                ((rows, local * inner_width), BF16),
                ((rows, LANES), F32),
                ((batch, slice_width), F32),
                ((local * inner_width, width), BF16),
            ],
            [VMEM] * (3 * n_ep + 4) + [HBM],
            (
                *pieces, *siblings, *mixed_all, ffn_gain[None], router, gate_w, up_w,
                pltpu.with_memory_space_constraint(expert_down, pltpu.HBM),
            ),
            [
                pltpu.VMEM((rows, width), F32),
                pltpu.VMEM((rows, width), BF16),
                pltpu.SemaphoreType.DMA((local,)),
            ],
            flops=4 * rows * width * inner_width * local,
        )

        give, shared = call(
            functools.partial(down_kernel, n_ep, n_z, False),
            [((rows, side), BF16), ((rows, shared_width), BF16)],
            [VMEM] * (n_ep + 4),
            (inner, shared_own, *shared_got, scales, down_w, shared_down_w),
            flops=rows * width * inner_width * local,
        )
        core = core_swap(give)
        (keep,) = call(
            functools.partial(down_kernel, n_ep, n_z, True),
            [((rows, side), F32)],
            [VMEM] * 4,
            (inner, shared, down_w, shared_down_w),
            flops=rows * width * inner_width * local,
        )
        own, *sent = call(
            functools.partial(merge_kernel, n_ep),
            [((batch, side), F32)] + [((batch, side), BF16)] * (n_ep - 1),
            [VMEM] * 2,
            (keep, core),
        )
        got = [ep_swap(sent[k - 1], k) for k in others]
        group = 4
        new_state, token = pl.pallas_call(
            functools.partial(update_kernel, group),
            out_shape=[
                jax.ShapeDtypeStruct(recurrent_state.shape, F32),
                jax.ShapeDtypeStruct((8, LANES), F32),
            ],
            in_specs=[VMEM] * 3,
            out_specs=[HBM, VMEM],
            scratch_shapes=[
                pltpu.VMEM(recurrent_state.shape, F32),
                pltpu.SemaphoreType.DMA((batch // group,)),
            ],
            cost_estimate=pl.CostEstimate(flops=1 << 26, bytes_accessed=0, transcendentals=0),
            compiler_params=pltpu.CompilerParams(vmem_limit_bytes=16 << 20),
        )(gates, state, own)
        base, *sent = call(
            functools.partial(gather_kernel, n_ep, n_z),
            [((batch, slice_width), F32)] + [((batch, slice_width), BF16)] * (n_z - 1),
            [VMEM] * (n_ep + 2),
            (own, *got, own_hidden, token),
            [pltpu.VMEM((batch, side), F32)],
        )
        got = [z_swap(sent[m - 1], m) for m in range(1, n_z)]
        (layer_out,) = call(
            finish_kernel, [((batch, slice_width), BF16)], [VMEM] * n_z, (base, *got)
        )
        return layer_out, new_state

    return body


def solution(mesh):
    body = make_body(mesh.shape["ep"], mesh.shape["tp"])

    return jax.shard_map(
        body,
        mesh=mesh,
        in_specs=(
            P("ep", None),
            P(),
            P("ep", "tp"),
            P("ep", "tp"),
            P("ep", "tp"),
            P("ep", "tp"),
            P("tp"),
            P("tp"),
            P("ep", "tp", None, None),
            P("tp", "ep"),
            P(),
            P(),
            P("ep", None),
            P("ep", None, "tp"),
            P("ep", None, "tp"),
            P("ep", "tp", None),
            P("ep", "tp"),
            P("ep", "tp"),
            P("tp", "ep"),
            P(),
        ),
        out_specs=(P("ep", "tp"), P("ep", "tp", None, None)),
        check_vma=False,
    )
```
